32 devices in a mesh: sp: 8 (over z, x), tp: 4 (over y, core).
Axes of the slice: x: 2, y: 2, z: 4, core: 2. Of those that a mesh axis runs over, the one named last changes fastest.
Arguments:
- resid: bfloat16 [2048, 4096], P('sp'), may hold values from -6 to 6
- queries: bfloat16 [2048, 3072], P('sp', 'tp'), may hold values from -1000 to 1000
- latent: bfloat16 [2048, 512], P('sp'), may hold values from -6 to 6
- rope_key: bfloat16 [2048, 64], P('sp'), may hold values from -6 to 6
- lat_gain: float32 [512], replicated, may hold values from 0.1 to 1.9
- kv_weight: bfloat16 [512, 4096], P(None, 'tp'), may hold values from -4 to 4
- out_gain: float32 [2048], P('tp'), may hold values from 0.1 to 1.9
- out_weight: bfloat16 [2048, 4096], P('tp'), may hold values from -0.125 to 0.125
- ffn_gain: float32 [4096], replicated, may hold values from 0.1 to 1.9
- gate_weight: bfloat16 [4096, 6144], P('sp', 'tp'), may hold values from -0.09375 to 0.09375
- up_weight: bfloat16 [4096, 6144], P('sp', 'tp'), may hold values from -0.09375 to 0.09375
- down_weight: bfloat16 [6144, 4096], P('tp', 'sp'), may hold values from -0.078125 to 0.078125
Outputs:
- result: bfloat16 [2048, 4096], P(('sp', 'tp'))
The draws below stay inside these ranges and needn't reach their ends.
All inputs are finite; a program needn't handle non-finite values.
Results may differ from the reference program's by a relative error of at most 0.018.
Values may be sent and summed in bfloat16 or wider, within the bound.
A program may use at most 192 MiB of HBM per device.

```python
import math
import jax
import jax.numpy as jnp
from jax import lax

D = 4096
HEADS = 16
NOPE = 128
ROPE = 64
VDIM = 128
KV_RANK = 512
FF = 6144
TOK_DEV = 256
TOKENS = 2048
N_TP = 4


def draw_pair(key):
    base = jax.random.fold_in(key, 7)
    key_one, key_two = jax.random.split(base, 2)
    width = NOPE + ROPE
    query = jax.random.truncated_normal(key_one, -6.0, 6.0, (TOKENS, HEADS, width), jnp.float32)
    rotary = jax.random.truncated_normal(key_two, -4.0, 4.0, (TOKENS, ROPE), jnp.float32)
    return (query.reshape(TOKENS, HEADS * width), rotary)


def draw_queries(key, part):
    return draw_pair(key)[0].astype(jnp.bfloat16)


def draw_rope_key(key, part):
    return draw_pair(key)[1].astype(jnp.bfloat16)


def draw_kv_weight(key, part):
    base = jax.random.fold_in(key, 11)
    shape = (KV_RANK, HEADS, NOPE + VDIM)
    matrix = jax.random.truncated_normal(base, -6.0, 6.0, shape, jnp.float32)
    ceiling = 3.0
    factor = ceiling ** (jnp.arange(HEADS, dtype=jnp.float32) / (HEADS - 1))
    scaled = jnp.concatenate([matrix[:, :, :NOPE], matrix[:, :, NOPE:] * factor[None, :, None]], axis=-1)
    return (scaled / math.sqrt(KV_RANK)).reshape(KV_RANK, HEADS * (NOPE + VDIM)).astype(jnp.bfloat16)


def shard_levels(rng, shape, pieces, low, top_value):
    level, own = 1.0, jax.random.fold_in(rng, 6)
    for dim, shards_of in pieces:
        heights = jnp.exp(jax.random.uniform(jax.random.fold_in(own, dim), (shards_of,), jnp.float32, low / len(pieces), top_value / len(pieces)))
        level = level * jnp.repeat(heights, shape[dim] // shards_of).reshape([-1 if axis == dim else 1 for axis in range(len(shape))])
    return level


def noise(own_key, dims, scale, reach, shards=(), kind=jnp.bfloat16):
    values = scale * jax.random.normal(own_key, dims, jnp.float32)
    if shards:
        values = values * shard_levels(own_key, dims, shards, -0.22, 0.18)
    return jnp.clip(values, -reach, reach).astype(kind)


def setup_inputs(seed: int = 0) -> dict:
    streams_of = jax.random.split(jax.random.key(seed), 13)
    return {
        "resid": noise(streams_of[0], (TOKENS, D), 1.0, 6.0, ((0, 8),)),
        "queries": draw_queries(jax.random.fold_in(streams_of[12], 71), 0),
        "latent": noise(streams_of[2], (TOKENS, KV_RANK), 1.0, 6.0, ((0, 8),)),
        "rope_key": draw_rope_key(jax.random.fold_in(streams_of[12], 71), 0),
        "lat_gain": jnp.clip(1.0 + 0.18 * jax.random.normal(streams_of[4], (KV_RANK,), jnp.float32), 0.1, 1.9),
        "kv_weight": draw_kv_weight(jax.random.fold_in(streams_of[12], 71), 0),
        "out_gain": jnp.clip(1.0 + 0.18 * jax.random.normal(streams_of[6], (HEADS * VDIM,), jnp.float32), 0.1, 1.9),
        "out_weight": noise(streams_of[7], (HEADS * VDIM, D), (HEADS * VDIM) ** -0.5, 0.125, ((0, 4),)),
        "ffn_gain": jnp.clip(1.0 + 0.18 * jax.random.normal(streams_of[8], (D,), jnp.float32), 0.1, 1.9),
        "gate_weight": noise(streams_of[9], (D, FF), D ** -0.5, 0.09375, ((0, 8), (1, 4))),
        "up_weight": noise(streams_of[10], (D, FF), D ** -0.5, 0.09375, ((0, 8), (1, 4))),
        "down_weight": noise(streams_of[11], (FF, D), FF ** -0.5, 0.078125, ((0, 4), (1, 8))),
    }


EPSILON = 1e-06
THETA = 10000.0

def rotate(values, places):
    half = values.shape[-1] // 2
    inverse = THETA ** (-jnp.arange(half, dtype=jnp.float32) / half)
    angle = places[..., None] * inverse
    cosine = jnp.cos(angle)
    sine = jnp.sin(angle)
    first = values[..., :half]
    second = values[..., half:]
    return jnp.concatenate([first * cosine - second * sine, first * sine + second * cosine], axis=-1)

def norm_rows(values, gain):
    wide = values.astype(jnp.float32)
    return wide * lax.rsqrt(lax.optimization_barrier(jnp.mean(wide * wide, axis=-1, keepdims=True)) + EPSILON) * gain.astype(jnp.float32)

def round_trip(values):
    return lax.optimization_barrier(values.astype(jnp.bfloat16)).astype(jnp.float32)

def reference(resid, queries, latent, rope_key, lat_gain, kv_weight, out_gain, out_weight, ffn_gain, gate_weight, up_weight, down_weight):
    total_rows = latent.shape[0]
    positions = jnp.arange(total_rows, dtype=jnp.int32)
    places = positions.astype(jnp.float32)
    normed = norm_rows(latent, lat_gain).astype(jnp.bfloat16)
    key_value = jnp.dot(normed, kv_weight, preferred_element_type=jnp.float32).astype(jnp.bfloat16)
    key_value = key_value.reshape(total_rows, HEADS, NOPE + VDIM).astype(jnp.float32)
    key_nope = key_value[:, :, :NOPE]
    values = key_value[:, :, NOPE:]
    key_rope = round_trip(rotate(rope_key.astype(jnp.float32), places))
    query = queries.reshape(total_rows, HEADS, NOPE + ROPE)
    query_nope = query[:, :, :NOPE].astype(jnp.float32)
    query_rope = round_trip(rotate(query[:, :, NOPE:].astype(jnp.float32), places[:, None]))
    scale = 1.0 / math.sqrt(NOPE + ROPE)
    blocks = total_rows // TOK_DEV

    def attend_block(index):
        first = (index * TOK_DEV).astype(jnp.int32)
        block_nope = lax.dynamic_slice_in_dim(query_nope, first, TOK_DEV, 0)
        block_rope = lax.dynamic_slice_in_dim(query_rope, first, TOK_DEV, 0)
        scores = jnp.einsum('qhd,khd->hqk', block_nope, key_nope) + jnp.einsum('qhr,kr->hqk', block_rope, key_rope)
        scores = scores * scale
        query_index = first + jnp.arange(TOK_DEV, dtype=jnp.int32)
        allowed = (positions[None, :] <= query_index[:, None])[None]
        scores = jnp.where(allowed, scores, -jnp.inf)
        highest = lax.optimization_barrier(jnp.max(scores, axis=-1, keepdims=True))
        weights = jnp.where(allowed, jnp.exp(scores - highest), 0.0)
        totals = lax.optimization_barrier(jnp.sum(weights, axis=-1))
        mixed = jnp.einsum('hqk,khd->qhd', round_trip(weights), values)
        return (mixed / jnp.transpose(totals)[:, :, None]).astype(jnp.bfloat16)
    attended = lax.map(attend_block, jnp.arange(blocks, dtype=jnp.int32))
    attended = attended.reshape(total_rows, HEADS * VDIM)
    normed_out = norm_rows(attended, out_gain).astype(jnp.bfloat16)
    group_width = HEADS * VDIM // N_TP
    attn_sum = jnp.zeros((total_rows, D), jnp.float32)
    for group in range(N_TP):
        lower = group * group_width
        part = jnp.dot(normed_out[:, lower:lower + group_width], out_weight[lower:lower + group_width], preferred_element_type=jnp.float32)
        attn_sum = attn_sum + round_trip(part)
    middle = (resid.astype(jnp.float32) + attn_sum).astype(jnp.bfloat16)
    normed_mid = norm_rows(middle, ffn_gain).astype(jnp.bfloat16)
    gate = jnp.dot(normed_mid, gate_weight, preferred_element_type=jnp.float32)
    upward = jnp.dot(normed_mid, up_weight, preferred_element_type=jnp.float32)
    hidden = (jax.nn.silu(gate) * upward).astype(jnp.bfloat16)
    group_units = FF // N_TP
    ffn_sum = jnp.zeros((total_rows, D), jnp.float32)
    for group in range(N_TP):
        lower = group * group_units
        part = jnp.dot(hidden[:, lower:lower + group_units], down_weight[lower:lower + group_units], preferred_element_type=jnp.float32)
        ffn_sum = ffn_sum + round_trip(part)
    return (middle.astype(jnp.float32) + ffn_sum).astype(jnp.bfloat16)
```

```python
import math

import jax
import jax.numpy as jnp
from jax import lax
from jax.experimental import pallas as pl
from jax.experimental.pallas import tpu as pltpu
from jax.sharding import PartitionSpec as P


HEADS = 16
NOPE = 128
ROPE = 64
VDIM = 128


EPSILON = 1e-06
THETA = 10000.0
LOWEST = -1e30
GROUP = 4


def rotate(values, places):
    half = values.shape[-1] // 2
    inverse = THETA ** (-jnp.arange(half, dtype=jnp.float32) / half)
    angle = places[..., None] * inverse
    cosine = jnp.cos(angle)
    sine = jnp.sin(angle)
    first = values[..., :half]
    second = values[..., half:]
    return jnp.concatenate(
        [first * cosine - second * sine, first * sine + second * cosine], axis=-1
    )


def norm_rows(values, gain):
    wide = values.astype(jnp.float32)
    return wide * lax.rsqrt(jnp.mean(wide * wide, axis=-1, keepdims=True) + EPSILON) * gain


def make_keys(latent_piece, rotary_piece, lat_gain, kv_weight, key_index):
    normed = norm_rows(latent_piece, lat_gain).astype(jnp.bfloat16)
    key_value = jnp.dot(normed, kv_weight, preferred_element_type=jnp.float32)
    key_value = key_value.astype(jnp.bfloat16)
    key_rope = rotate(rotary_piece.astype(jnp.float32), key_index.astype(jnp.float32)).astype(
        jnp.bfloat16
    )
    return (key_value, key_rope)


def to_near(values, flip):
    ranks = lax.axis_size("sp")
    return lax.ppermute(values, "sp", [(rank, rank ^ flip) for rank in range(ranks)])


def to_high(values, step, ranks):
    if step % (ranks // GROUP) == 0:
        return values
    return lax.ppermute(
        values, "sp", [(rank, (rank + step * GROUP) % ranks) for rank in range(ranks)]
    )


def reorder(blocks, place):
    bit = 1
    while bit < len(blocks):
        swap = place // bit % 2 == 1
        blocks = [jnp.where(swap, blocks[j ^ bit], blocks[j]) for j in range(len(blocks))]
        bit *= 2
    return blocks


def by_distance(values, place):
    return jnp.concatenate(reorder(jnp.split(values, GROUP, axis=1), place), axis=1)


def to_column(values, bit):
    columns = lax.axis_size("tp")
    return lax.ppermute(values, "tp", [(column, column ^ bit) for column in range(columns)])


def gather_columns(values):
    rows = values.shape[0]
    held = {0: values}
    bit = lax.axis_size("tp") // 2
    while bit:
        keys = sorted(held)
        theirs = to_column(jnp.concatenate([held[key] for key in keys], axis=0), bit)
        for at, key in enumerate(keys):
            held[key + bit] = theirs[at * rows : (at + 1) * rows]
        bit //= 2
    return jnp.concatenate([held[key] for key in sorted(held)], axis=0)


def scatter_columns(values):
    columns = lax.axis_size("tp")
    blocks = dict(enumerate(jnp.split(values, columns, axis=0)))
    bit = 1
    while bit < columns:
        mine = [key for key in sorted(blocks) if not key & bit]
        theirs = to_column(jnp.concatenate([blocks[key + bit] for key in mine], axis=0), bit)
        theirs = jnp.split(theirs, len(mine), axis=0)
        blocks = {
            key: (blocks[key].astype(jnp.float32) + piece.astype(jnp.float32)).astype(jnp.bfloat16)
            for key, piece in zip(mine, theirs)
        }
        bit *= 2
    return blocks[0]


def near_weights(gate, up, down):
    gate_one = to_near(gate, 1)
    up_two = to_near(up, 2)
    up_one = to_near(up, 1)
    gate_two = to_near(gate, 2)
    gate_both = to_near(gate_one, 2)
    up_both = to_near(up_two, 1)
    down, gate_both, up_both = lax.optimization_barrier((down, gate_both, up_both))
    half = down.shape[0] // 2
    down_one = to_near(down, 1)
    down_two = to_near(down, 2)
    far = [to_near(down_one[:half], 2), to_near(down_two[half:], 1)]
    down_both = jnp.concatenate(far, axis=0)
    return (
        (gate, gate_one, gate_two, gate_both),
        (up, up_one, up_two, up_both),
        (down, down_one, down_two, down_both),
    )


def blocks_dot(rows, weights, block):
    return sum(
        jnp.dot(
            rows[:, place * block : (place + 1) * block], weight, preferred_element_type=jnp.float32
        )
        for place, weight in enumerate(weights)
    )


def plain_body(
    resid,
    queries,
    latent,
    rope_key,
    lat_gain,
    kv_weight,
    out_gain,
    out_weight,
    ffn_gain,
    gate_weight,
    up_weight,
    down_weight,
):
    gate_blocks, up_blocks, down_blocks = near_weights(gate_weight, up_weight, down_weight)
    rows_here = resid.shape[0]
    first_row = lax.axis_index("sp") * rows_here
    heads_here = queries.shape[1] // (NOPE + ROPE)
    columns = lax.axis_size("tp")
    column = lax.axis_index("tp")
    share = rows_here // columns
    query = jnp.concatenate(reorder(jnp.split(queries, columns, axis=0), column), axis=0)
    query = query.reshape(rows_here, heads_here, NOPE + ROPE)
    within = jnp.arange(rows_here, dtype=jnp.int32)
    own_columns = (within // share) ^ column
    query_index = first_row + own_columns * share + within % share
    query_nope = query[:, :, :NOPE]
    query_rope = rotate(
        query[:, :, NOPE:].astype(jnp.float32), query_index.astype(jnp.float32)[:, None]
    ).astype(jnp.bfloat16)
    scale = 1.0 / math.sqrt(NOPE + ROPE)

    def accumulate(state, key_value, key_rope):
        running_max, running_sum, weighted = state
        length = key_value.shape[0]
        key_value = key_value.reshape(length, heads_here, NOPE + VDIM)
        scores = jnp.einsum(
            "qhd,khd->hqk", query_nope, key_value[:, :, :NOPE], preferred_element_type=jnp.float32
        )
        scores = (
            scores
            + jnp.einsum("qhr,kr->hqk", query_rope, key_rope, preferred_element_type=jnp.float32)
        ) * scale
        allowed = (key_index[None, :] <= query_index[:, None])[None]
        scores = jnp.where(allowed, scores, LOWEST)
        new_max = jnp.maximum(running_max, jnp.max(scores, axis=-1))
        weights = jnp.where(allowed, jnp.exp(scores - new_max[:, :, None]), 0.0)
        running_sum = jnp.sum(weights, axis=-1)
        added = jnp.einsum(
            "hqk,khd->qhd",
            weights.astype(jnp.bfloat16),
            key_value[:, :, NOPE:],
            preferred_element_type=jnp.float32,
        )
        weighted = added
        return (new_max, running_sum, weighted)

    initial = (
        jnp.full((heads_here, rows_here), LOWEST, jnp.float32),
        jnp.zeros((heads_here, rows_here), jnp.float32),
        jnp.zeros((rows_here, heads_here, VDIM), jnp.float32),
    )
    ranks = lax.axis_size("sp")
    rank = lax.axis_index("sp")
    both = jnp.concatenate([latent, rope_key], axis=1)
    both = lax.dynamic_slice_in_dim(both, column * share, share, 0)
    pieces = [both]
    for step in range(1, ranks):
        onward = [(source, source + step) for source in range(ranks - step)]
        pieces.append(lax.ppermute(both, "sp", onward))
    both = gather_columns(jnp.concatenate(pieces, axis=0))
    within = jnp.arange(both.shape[0], dtype=jnp.int32)
    source = (rank - within // share % ranks + ranks) % ranks
    key_index = source * rows_here + ((within // (share * ranks)) ^ column) * share + within % share
    pieces = (both[:, : latent.shape[1]], both[:, latent.shape[1] :])

    def update(state):
        key_value, key_rope = make_keys(pieces[0], pieces[1], lat_gain, kv_weight, key_index)
        return accumulate(state, key_value, key_rope)

    _, running_sum, weighted = update(initial)
    attended = (weighted / jnp.transpose(running_sum)[:, :, None]).astype(jnp.bfloat16)
    attended_float = attended.reshape(rows_here, heads_here * VDIM).astype(jnp.float32)
    squares = jnp.split(jnp.sum(attended_float * attended_float, axis=1), columns)
    squares = lax.psum(jnp.concatenate(reorder(squares, column)), "tp")
    squares = jnp.concatenate(reorder(jnp.split(squares, columns), column))
    normed_out = attended_float * lax.rsqrt(squares / (HEADS * VDIM) + EPSILON)[:, None] * out_gain
    normed_out = normed_out.astype(jnp.bfloat16)
    own_first = lax.axis_index("tp") * share
    projected = jnp.dot(normed_out, out_weight, preferred_element_type=jnp.float32)
    projected = projected.astype(jnp.bfloat16)
    attn_sum = scatter_columns(projected).astype(jnp.float32)
    own_resid = lax.dynamic_slice_in_dim(resid, own_first, share, 0)
    middle = (own_resid.astype(jnp.float32) + attn_sum).astype(jnp.bfloat16)
    highs = ranks // GROUP
    high = rank // GROUP
    place = rank % GROUP
    width = resid.shape[1]
    block = width // ranks
    wide = GROUP * block
    mids = norm_rows(middle, ffn_gain).astype(jnp.bfloat16)
    mids = [
        to_high(
            by_distance(
                lax.dynamic_slice_in_dim(mids, (high + step) % highs * wide, wide, 1), place
            ),
            step,
            ranks,
        )
        for step in range(highs)
    ]
    mids = [gather_columns(piece) for piece in mids]
    gates, ups = None, None
    for step in list(range(1, highs)) + [0]:
        piece = mids[step]
        gate = blocks_dot(piece, gate_blocks, block)
        up = blocks_dot(piece, up_blocks, block)
        if step:
            gate = to_high(gate.astype(jnp.bfloat16), highs - step, ranks).astype(jnp.float32)
            up = to_high(up.astype(jnp.bfloat16), highs - step, ranks).astype(jnp.float32)
        gates = gate if gates is None else gates + gate
        ups = up if ups is None else ups + up
    hidden = (jax.nn.silu(gates) * ups).astype(jnp.bfloat16)
    received = [to_high(hidden, step, ranks) for step in range(highs)]
    terms = []
    for step in range(highs):
        partial = jnp.concatenate(
            [
                jnp.dot(received[step], weight, preferred_element_type=jnp.float32).astype(
                    jnp.bfloat16
                )
                for weight in down_blocks
            ],
            axis=1,
        )
        partial = to_high(scatter_columns(partial), highs - step, ranks)
        terms.append(by_distance(partial, place))
    terms = jnp.concatenate(terms, axis=1)
    ffn_sum = jnp.concatenate(
        [
            lax.dynamic_slice_in_dim(terms, (index - high + highs) % highs * wide, wide, 1)
            for index in range(highs)
        ],
        axis=1,
    ).astype(jnp.float32)
    return (middle.astype(jnp.float32) + ffn_sum).astype(jnp.bfloat16)


LANES = 128
PAIR = 2
LINE = 4
COLUMNS = 4
MESH = pl.DeviceIdType.MESH


def whole_step(
    lat_ref,
    query_ref,
    resid_ref,
    out_gain_ref,
    ffn_gain_ref,
    kv_hbm,
    out_hbm,
    gate_hbm,
    up_hbm,
    down_hbm,
    result_ref,
    lat_buf,
    kv_w,
    out_w,
    gate_up,
    down,
    act,
    hidden,
    top,
    norm,
    acc,
    stats_mine,
    stats_in,
    partial,
    core_in,
    near_out,
    near_in,
    line_out,
    line_in,
    middle,
    total,
    local_sem,
    lat_send,
    lat_recv,
    lat_spread_send,
    lat_spread_recv,
    turn_send,
    turn_recv,
    pair_send,
    pair_recv,
    act_line_send,
    act_line_recv,
    act_spread_send,
    act_spread_recv,
    stat_send,
    stat_recv,
    core_send,
    core_recv,
    near_send,
    near_recv,
    line_send,
    line_recv,
):
    rank = lax.axis_index("sp")
    col = lax.axis_index("tp")
    ranks = lat_buf.shape[0]
    rows = lat_buf.shape[1]
    share = lat_ref.shape[0]
    width = resid_ref.shape[1]
    units = hidden.shape[1]
    block = gate_hbm.shape[0]
    latent = kv_w.shape[0]
    heads = query_ref.shape[1] // (2 * LANES)
    z = rank // PAIR
    x = rank % PAIR
    mate = z * PAIR + (PAIR - 1 - x)
    inner = ((z + 1) // 2) % 2
    z_flips = [z, z + 1 - 2 * (z % 2), (z + 2) % LINE, LINE - 1 - z]
    col_flips = [col, col + 1 - 2 * (col % 2), (col + 2) % COLUMNS, COLUMNS - 1 - col]
    pending = []

    def remote(src, dst, send, recv, sp=None, tp=None):
        target = (rank if sp is None else sp, col if tp is None else tp)
        return pltpu.make_async_remote_copy(
            src_ref=src, dst_ref=dst, send_sem=send, recv_sem=recv, device_id=target,
            device_id_type=MESH,
        )

    def arrived(dst, recv):
        remote(dst, dst, recv, recv, tp=col_flips[1]).wait_recv()

    def send(copy, when=None):
        if when is None:
            copy.start()
        else:
            pl.when(when)(copy.start)
        pending.append((copy, when))

    barrier = pltpu.get_barrier_semaphore()
    for step in range(1, ranks):
        pl.semaphore_signal(
            barrier, inc=1, device_id=((rank + step) % ranks, col), device_id_type=MESH
        )
    for flip in col_flips[1:]:
        pl.semaphore_signal(barrier, inc=1, device_id=(rank, flip), device_id_type=MESH)
    pl.semaphore_wait(barrier, ranks - 1 + COLUMNS - 1)

    def lat_piece(source, column):
        return lat_buf.at[source, pl.ds(pl.multiple_of(column * share, share), share), :]

    def lat_spread(source, piece, flip, slot):
        return remote(
            piece, lat_piece(source, col_flips[slot - flip]),
            lat_spread_send.at[source, slot - 1], lat_spread_recv.at[source, slot - 1],
            tp=col_flips[flip],
        )

    for step in range(1, ranks):
        send(
            remote(
                lat_ref, lat_piece(rank, col), lat_send.at[step - 1], lat_recv.at[rank],
                sp=(rank + step) % ranks,
            ),
            rank + step < ranks,
        )
    lat_spread(rank, lat_ref, 2, 2).start()
    lat_spread(rank, lat_ref, 1, 1).start()
    lat_buf[rank, pl.ds(pl.multiple_of(col * share, share), share), :] = lat_ref[...]

    def region(kind, source):
        at = pl.multiple_of(source * block, block)
        if kind == 2:
            return down.at[:, pl.ds(at, block)]
        return gate_up.at[pl.ds(at, block), pl.ds(kind * units, units)]

    def own_part(kind, place):
        at = pl.multiple_of(place * units, units)
        if kind == 2:
            return down_hbm.at[pl.ds(at, units), :]
        return (gate_hbm, up_hbm)[kind].at[:, pl.ds(at, units)]

    def local(src, dst, slot):
        copy = pltpu.make_async_copy(src, dst, local_sem.at[slot])
        copy.start()
        return copy

    kv_copy = local(kv_hbm, kv_w, 0)
    out_copy = local(out_hbm, out_w, 1)
    own_copies = [local(own_part(kind, z), region(kind, rank), 2 + kind) for kind in range(3)]

    def turn(kind):
        for k in range(1, LINE):
            send(
                remote(
                    own_part(kind, z_flips[k]), region(kind, rank), turn_send.at[kind, k],
                    turn_recv.at[kind, k], sp=z_flips[k] * PAIR + x,
                )
            )

    def pump(kind, k):
        here = region(kind, z_flips[k] * PAIR + x)
        if k:
            arrived(here, turn_recv.at[kind, k])
        send(
            remote(
                here if k else own_part(kind, z), here, pair_send.at[kind, k],
                pair_recv.at[kind, k], sp=mate,
            )
        )

    def paired(kind):
        for k in range(LINE):
            arrived(region(kind, z_flips[k] * PAIR + (PAIR - 1 - x)), pair_recv.at[kind, k])

    turn(0)
    turn(1)
    pump(0, 0)
    pump(1, 0)

    top[...] = jnp.full(top.shape, LOWEST, jnp.float32)
    norm[...] = jnp.zeros(norm.shape, jnp.float32)
    acc[...] = jnp.zeros(acc.shape, jnp.float32)
    scale = 1.0 / math.sqrt(NOPE + ROPE)
    kv_copy.wait()

    def attend(index, carry):
        source = rank - index

        @pl.when(index < rank)
        def _():
            arrived(lat_piece(source - 1, col), lat_recv.at[source - 1])
            piece = lat_piece(source - 1, col)
            lat_spread(source - 1, piece, 2, 2).start()
            lat_spread(source - 1, piece, 1, 1).start()

        arrived(lat_piece(source, col_flips[2]), lat_spread_recv.at[source, 1])
        lat_spread(source, lat_piece(source, col_flips[2]), 1, 3).start()
        arrived(lat_piece(source, col_flips[1]), lat_spread_recv.at[source, 0])
        arrived(lat_piece(source, col_flips[3]), lat_spread_recv.at[source, 2])
        key_value = jnp.dot(
            lat_buf[source, :, :latent], kv_w[...], preferred_element_type=jnp.float32
        ).astype(jnp.bfloat16)
        key_rope = lat_buf[source, :, latent:]
        row_of = lax.broadcasted_iota(jnp.int32, (rows, rows), 0) + index * rows
        allowed = lax.broadcasted_iota(jnp.int32, (rows, rows), 1) <= row_of
        for head in range(heads):
            at = head * (NOPE + VDIM)
            keys = jnp.concatenate([key_value[:, at : at + NOPE], key_rope], axis=1)
            scores = lax.dot_general(
                query_ref[:, head * 2 * LANES : (head + 1) * 2 * LANES], keys,
                (((1,), (1,)), ((), ())), preferred_element_type=jnp.float32,
            )
            scores = jnp.where(allowed, scores * scale, LOWEST)
            old = top[head]
            new = jnp.maximum(old, jnp.max(scores, axis=1, keepdims=True))
            weights = jnp.exp(scores - new[:, :1])
            fade = jnp.exp(old - new)
            top[head] = new
            norm[head] = norm[head] * fade + jnp.sum(weights, axis=1, keepdims=True)
            across = slice(head * VDIM, (head + 1) * VDIM)
            acc[:, across] = acc[:, across] * fade + jnp.dot(
                weights.astype(jnp.bfloat16), key_value[:, at + NOPE : at + NOPE + VDIM],
                preferred_element_type=jnp.float32,
            )
        return carry

    lax.fori_loop(0, rank + 1, attend, 0)
    for kind, k in ((0, 1), (1, 1), (0, 2)):
        pump(kind, k)

    squares = jnp.zeros((rows, 1), jnp.float32)
    attended = []
    for head in range(heads):
        across = slice(head * VDIM, (head + 1) * VDIM)
        part = (acc[:, across] / norm[head]).astype(jnp.bfloat16).astype(jnp.float32)
        squares = squares + jnp.sum(part * part, axis=1, keepdims=True)
        attended.append((part * out_gain_ref[:, across]).astype(jnp.bfloat16))
    attended = jnp.concatenate(attended, axis=1)
    stats_mine[...] = jnp.broadcast_to(squares, stats_mine.shape)

    chunk = 4 * LANES
    chunks = width // chunk

    def piece_of(ref, slot, column):
        return ref.at[slot, pl.ds(pl.multiple_of(column * share, share), share), :]

    def project(slot, left, right):
        def one(index, carry):
            at = pl.ds(pl.multiple_of(index * chunk, chunk), chunk)
            partial[slot, :, at] = jnp.dot(
                left, right[:, at], preferred_element_type=jnp.float32
            ).astype(jnp.bfloat16)
            return carry

        lax.fori_loop(0, chunks, one, 0)

    def each_chunk(work):
        def one(index, carry):
            work(pl.ds(pl.multiple_of(index * chunk, chunk), chunk))
            return carry

        lax.fori_loop(0, chunks, one, 0)

    def fold(slot):
        send(
            remote(
                piece_of(partial, slot, col_flips[3]), core_in.at[slot, 1],
                core_send.at[slot, 1], core_recv.at[slot, 1], tp=col_flips[1],
            )
        )
        send(
            remote(
                piece_of(partial, slot, col_flips[1]), core_in.at[slot, 0],
                core_send.at[slot, 0], core_recv.at[slot, 0], tp=col_flips[1],
            )
        )
        arrived(core_in.at[slot, 1], core_recv.at[slot, 1])

        def add(at):
            theirs = partial[
                slot, pl.ds(pl.multiple_of(col_flips[2] * share, share), share), at
            ].astype(jnp.float32)
            near_out[slot, :, at] = (theirs + core_in[slot, 1, :, at].astype(jnp.float32)).astype(
                jnp.bfloat16
            )

        each_chunk(add)
        send(
            remote(
                near_out.at[slot], near_in.at[slot], near_send.at[slot], near_recv.at[slot],
                tp=col_flips[2],
            )
        )
        arrived(core_in.at[slot, 0], core_recv.at[slot, 0])

    def folded(slot):
        arrived(near_in.at[slot], near_recv.at[slot])

        def add(at):
            mine = partial[slot, pl.ds(pl.multiple_of(col * share, share), share), at]
            total[:, at] = (
                mine.astype(jnp.float32)
                + core_in[slot, 0, :, at].astype(jnp.float32)
                + near_in[slot, :, at].astype(jnp.float32)
            )

        each_chunk(add)

    out_copy.wait()
    first = LINE
    for m in range(1, COLUMNS):
        send(
            remote(
                stats_mine.at[pl.ds(pl.multiple_of(col_flips[m] * share, share), share), :],
                stats_in.at[m - 1], stat_send.at[m - 1], stat_recv.at[m - 1], tp=col_flips[m],
            )
        )
    project(first, attended, out_w)
    fold(first)
    for kind, k in ((1, 2), (0, 3)):
        pump(kind, k)
    squares = stats_mine[pl.ds(pl.multiple_of(col * share, share), share), :]
    for m in range(1, COLUMNS):
        arrived(stats_in.at[m - 1], stat_recv.at[m - 1])
        squares = squares + stats_in[m - 1]
    factor = lax.rsqrt(squares / (HEADS * VDIM) + EPSILON)[:, :1]
    folded(first)
    squares = jnp.zeros((share, 1), jnp.float32)
    for index in range(chunks):
        at = slice(index * chunk, (index + 1) * chunk)
        mid = (resid_ref[:, at].astype(jnp.float32) + total[:, at] * factor).astype(jnp.bfloat16)
        middle[:, at] = mid
        mid = mid.astype(jnp.float32)
        squares = squares + jnp.sum(mid * mid, axis=1, keepdims=True)
    factor = lax.rsqrt(squares / width + EPSILON)

    def act_piece(place, column):
        at = pl.multiple_of(place * rows + column * share, share)
        return act.at[pl.ds(at, share), :]

    own_rows = pl.ds(pl.multiple_of(z * rows + col * share, share), share)
    for index in range(chunks):
        at = slice(index * chunk, (index + 1) * chunk)
        act[own_rows, at] = (
            middle[:, at].astype(jnp.float32) * factor * ffn_gain_ref[:, at]
        ).astype(jnp.bfloat16)

    def up_line(src, dst, send_sem, recv_sem, when):
        send(remote(src, dst, send_sem, recv_sem, sp=(rank + PAIR) % ranks), when)

    def down_line(src, dst, send_sem, recv_sem, when):
        send(remote(src, dst, send_sem, recv_sem, sp=(rank + ranks - PAIR) % ranks), when)

    def act_spread(place, index, flip, slot):
        piece = act_piece(place, col_flips[slot - flip])
        send(
            remote(
                piece, piece, act_spread_send.at[index, slot - 1],
                act_spread_recv.at[index, slot - 1], tp=col_flips[flip],
            )
        )

    mine = act_piece(z, col)
    up_line(mine, mine, act_line_send.at[0], act_line_recv.at[z], z < LINE - 1)
    down_line(mine, mine, act_line_send.at[1], act_line_recv.at[z], z > 0)
    act_spread(z, 0, 2, 2)
    act_spread(z, 0, 1, 1)
    pump(1, 3)
    order = [
        z,
        z_flips[1],
        z_flips[2] * (1 - inner) + z_flips[3] * inner,
        z_flips[3] * (1 - inner) + z_flips[2] * inner,
    ]
    for index in range(LINE):
        place = order[index]
        if index < LINE - 1:
            nearer = order[index + 1]
            piece = act_piece(nearer, col)
            arrived(piece, act_line_recv.at[nearer])
            up_line(
                piece, piece, act_line_send.at[2 + 2 * index], act_line_recv.at[nearer],
                (nearer < z) & (z < LINE - 1),
            )
            down_line(
                piece, piece, act_line_send.at[3 + 2 * index], act_line_recv.at[nearer],
                (nearer > z) & (z > 0),
            )
            act_spread(nearer, index + 1, 2, 2)
            act_spread(nearer, index + 1, 1, 1)
        if index == LINE - 2:
            turn(2)
            pump(2, 0)
        if index == 0:
            own_copies[0].wait()
            own_copies[1].wait()
            paired(0)
            paired(1)
        arrived(act_piece(place, col_flips[2]), act_spread_recv.at[index, 1])
        act_spread(place, index, 1, 3)
        arrived(act_piece(place, col_flips[1]), act_spread_recv.at[index, 0])
        arrived(act_piece(place, col_flips[3]), act_spread_recv.at[index, 2])
        here = pl.ds(pl.multiple_of(place * rows, rows), rows)
        both = jnp.dot(act[here, :], gate_up[...], preferred_element_type=jnp.float32)
        gate = both[:, :units]
        hidden[here, :] = (gate / (1.0 + jnp.exp(-gate)) * both[:, units:]).astype(jnp.bfloat16)

    for k in range(1, LINE):
        pump(2, k)
    own_copies[2].wait()
    paired(2)

    def start_rows(slot):
        place = z_flips[LINE - 1 - slot]
        left = hidden[pl.ds(pl.multiple_of(place * rows, rows), rows), :]
        project(slot, left, down)
        fold(slot)

    def add_line(slot):
        def add(at):
            total[:, at] = total[:, at] + line_in[slot, :, at].astype(jnp.float32)

        each_chunk(add)

    def pass_rows(slot):
        place = z_flips[LINE - 1 - slot]
        folded(slot)

        @pl.when(((place > z) & (z > 0)) | ((place < z) & (z < LINE - 1)))
        def _():
            arrived(line_in.at[place], line_recv.at[place])
            add_line(place)

        def keep(at):
            line_out[slot, :, at] = total[:, at].astype(jnp.bfloat16)

        each_chunk(keep)
        up_line(
            line_out.at[slot], line_in.at[place], line_send.at[slot, 0], line_recv.at[place],
            place > z,
        )
        last = jnp.where(place == z - 1, LINE, place)
        down_line(
            line_out.at[slot], line_in.at[last], line_send.at[slot, 1], line_recv.at[last],
            place < z,
        )

    start_rows(0)
    start_rows(1)
    pass_rows(0)
    start_rows(2)
    pass_rows(1)
    start_rows(3)
    pass_rows(2)
    folded(LINE - 1)

    @pl.when(z > 0)
    def _():
        arrived(line_in.at[z], line_recv.at[z])
        add_line(z)

    @pl.when(z < LINE - 1)
    def _():
        arrived(line_in.at[LINE], line_recv.at[LINE])
        add_line(LINE)

    def finish(at):
        result_ref[:, at] = (middle[:, at].astype(jnp.float32) + total[:, at]).astype(jnp.bfloat16)

    each_chunk(finish)

    for copy, when in pending:
        if when is None:
            copy.wait_send()
        else:
            pl.when(when)(copy.wait_send)

    def drain(source, carry):
        piece = lat_piece(source, col)
        for slot in range(COLUMNS - 1):
            remote(
                piece, piece, lat_spread_send.at[source, slot], lat_spread_send.at[source, slot],
                tp=col_flips[1],
            ).wait_send()
        return carry

    lax.fori_loop(0, rank + 1, drain, 0)


def fused_body(
    resid,
    queries,
    latent,
    rope_key,
    lat_gain,
    kv_weight,
    out_gain,
    out_weight,
    ffn_gain,
    gate_weight,
    up_weight,
    down_weight,
):
    ranks, columns = lax.axis_size("sp"), lax.axis_size("tp")
    rank, column = lax.axis_index("sp"), lax.axis_index("tp")
    rows, width = resid.shape
    share = rows // columns
    heads = queries.shape[1] // (NOPE + ROPE)
    units = gate_weight.shape[1] // LINE
    block = gate_weight.shape[0]
    own_first = column * share
    first_row = rank * rows

    def mine(values):
        return lax.dynamic_slice_in_dim(values, own_first, share, 0)

    places = (first_row + jnp.arange(rows, dtype=jnp.int32)).astype(jnp.float32)
    normed = norm_rows(mine(latent), lat_gain).astype(jnp.bfloat16)
    key_rope = rotate(mine(rope_key).astype(jnp.float32), mine(places)).astype(jnp.bfloat16)
    message = jnp.concatenate([normed, key_rope, jnp.zeros_like(key_rope)], axis=1)
    query = queries.reshape(rows, heads, NOPE + ROPE)
    query_rope = rotate(query[:, :, NOPE:].astype(jnp.float32), places[:, None]).astype(
        jnp.bfloat16
    )
    query = jnp.concatenate([query[:, :, :NOPE], query_rope, jnp.zeros_like(query_rope)], axis=2)
    query = query.reshape(rows, heads * 2 * LANES)
    bf, f32 = jnp.bfloat16, jnp.float32
    dma = pltpu.SemaphoreType.DMA
    slots = LINE + 1
    vmem = pl.BlockSpec(memory_space=pltpu.VMEM)
    anywhere = pl.BlockSpec(memory_space=pl.ANY)
    return pl.pallas_call(
        whole_step,
        out_shape=jax.ShapeDtypeStruct((share, width), bf),
        in_specs=[vmem] * 5 + [anywhere] * 5,
        out_specs=vmem,
        scratch_shapes=[
            pltpu.VMEM((ranks, rows, message.shape[1]), bf),
            pltpu.VMEM(kv_weight.shape, bf),
            pltpu.VMEM(out_weight.shape, bf),
            pltpu.VMEM((ranks * block, 2 * units), bf),
            pltpu.VMEM((units, ranks * down_weight.shape[1]), bf),
            pltpu.VMEM((LINE * rows, width), bf),
            pltpu.VMEM((LINE * rows, units), bf),
            pltpu.VMEM((heads, rows, LANES), f32),
            pltpu.VMEM((heads, rows, LANES), f32),
            pltpu.VMEM((rows, heads * VDIM), f32),
            pltpu.VMEM((rows, LANES), f32),
            pltpu.VMEM((columns - 1, share, LANES), f32),
            pltpu.VMEM((slots, rows, width), bf),
            pltpu.VMEM((slots, 2, share, width), bf),
            pltpu.VMEM((slots, share, width), bf),
            pltpu.VMEM((slots, share, width), bf),
            pltpu.VMEM((LINE, share, width), bf),
            pltpu.VMEM((slots, share, width), bf),
            pltpu.VMEM((share, width), bf),
            pltpu.VMEM((share, width), f32),
            dma((5,)),
            dma((ranks - 1,)),
            dma((ranks,)),
            dma((ranks, columns - 1)),
            dma((ranks, columns - 1)),
            dma((3, LINE)),
            dma((3, LINE)),
            dma((3, LINE)),
            dma((3, LINE)),
            dma((2 * LINE,)),
            dma((LINE,)),
            dma((LINE, columns - 1)),
            dma((LINE, columns - 1)),
            dma((columns - 1,)),
            dma((columns - 1,)),
            dma((slots, 2)),
            dma((slots, 2)),
            dma((slots,)),
            dma((slots,)),
            dma((LINE, 2)),
            dma((slots,)),
        ],
        compiler_params=pltpu.CompilerParams(
            collective_id=0, has_side_effects=True, vmem_limit_bytes=66 * 1024 * 1000
        ),
    )(
        message,
        query,
        mine(resid),
        out_gain.reshape(1, -1),
        ffn_gain.reshape(1, -1),
        kv_weight,
        out_weight,
        gate_weight,
        up_weight,
        down_weight,
    )


def solution(mesh):
    placed = (
        P("sp", None),
        P("sp", "tp"),
        P("sp", None),
        P("sp", None),
        P(),
        P(None, "tp"),
        P("tp"),
        P("tp", None),
        P(),
        P("sp", "tp"),
        P("sp", "tp"),
        P("tp", "sp"),
    )

    def mapped(function):
        return jax.shard_map(
            function, mesh=mesh, in_specs=placed, out_specs=P(("sp", "tp"), None), check_vma=False
        )

    if mesh.shape["sp"] == PAIR * LINE and mesh.shape["tp"] == COLUMNS:
        return mapped(fused_body)
    return mapped(plain_body)
```

```python
import math

import jax
import jax.numpy as jnp
from jax import lax
from jax.experimental import pallas as pl
from jax.experimental.pallas import tpu as pltpu
from jax.sharding import PartitionSpec as P


HEADS = 16
NOPE = 128
ROPE = 64
VDIM = 128


EPSILON = 1e-06
THETA = 10000.0
LOWEST = -1e30
GROUP = 4


def rotate(values, places):
    half = values.shape[-1] // 2
    inverse = THETA ** (-jnp.arange(half, dtype=jnp.float32) / half)
    angle = places[..., None] * inverse
    cosine = jnp.cos(angle)
    sine = jnp.sin(angle)
    first = values[..., :half]
    second = values[..., half:]
    return jnp.concatenate(
        [first * cosine - second * sine, first * sine + second * cosine], axis=-1
    )


def norm_rows(values, gain):
    wide = values.astype(jnp.float32)
    return wide * lax.rsqrt(jnp.mean(wide * wide, axis=-1, keepdims=True) + EPSILON) * gain


def make_keys(latent_piece, rotary_piece, lat_gain, kv_weight, key_index):
    normed = norm_rows(latent_piece, lat_gain).astype(jnp.bfloat16)
    key_value = jnp.dot(normed, kv_weight, preferred_element_type=jnp.float32)
    key_value = key_value.astype(jnp.bfloat16)
    key_rope = rotate(rotary_piece.astype(jnp.float32), key_index.astype(jnp.float32)).astype(
        jnp.bfloat16
    )
    return (key_value, key_rope)


def to_near(values, flip):
    ranks = lax.axis_size("sp")
    return lax.ppermute(values, "sp", [(rank, rank ^ flip) for rank in range(ranks)])


def to_high(values, step, ranks):
    if step % (ranks // GROUP) == 0:
        return values
    return lax.ppermute(
        values, "sp", [(rank, (rank + step * GROUP) % ranks) for rank in range(ranks)]
    )


def reorder(blocks, place):
    bit = 1
    while bit < len(blocks):
        swap = place // bit % 2 == 1
        blocks = [jnp.where(swap, blocks[j ^ bit], blocks[j]) for j in range(len(blocks))]
        bit *= 2
    return blocks


def by_distance(values, place):
    return jnp.concatenate(reorder(jnp.split(values, GROUP, axis=1), place), axis=1)


def to_column(values, bit):
    columns = lax.axis_size("tp")
    return lax.ppermute(values, "tp", [(column, column ^ bit) for column in range(columns)])


def gather_columns(values):
    rows = values.shape[0]
    held = {0: values}
    bit = lax.axis_size("tp") // 2
    while bit:
        keys = sorted(held)
        theirs = to_column(jnp.concatenate([held[key] for key in keys], axis=0), bit)
        for at, key in enumerate(keys):
            held[key + bit] = theirs[at * rows : (at + 1) * rows]
        bit //= 2
    return jnp.concatenate([held[key] for key in sorted(held)], axis=0)


def scatter_columns(values):
    columns = lax.axis_size("tp")
    blocks = dict(enumerate(jnp.split(values, columns, axis=0)))
    bit = 1
    while bit < columns:
        mine = [key for key in sorted(blocks) if not key & bit]
        theirs = to_column(jnp.concatenate([blocks[key + bit] for key in mine], axis=0), bit)
        theirs = jnp.split(theirs, len(mine), axis=0)
        blocks = {
            key: (blocks[key].astype(jnp.float32) + piece.astype(jnp.float32)).astype(jnp.bfloat16)
            for key, piece in zip(mine, theirs)
        }
        bit *= 2
    return blocks[0]


def near_weights(gate, up, down):
    gate_one = to_near(gate, 1)
    up_two = to_near(up, 2)
    up_one = to_near(up, 1)
    gate_two = to_near(gate, 2)
    gate_both = to_near(gate_one, 2)
    up_both = to_near(up_two, 1)
    down, gate_both, up_both = lax.optimization_barrier((down, gate_both, up_both))
    half = down.shape[0] // 2
    down_one = to_near(down, 1)
    down_two = to_near(down, 2)
    far = [to_near(down_one[:half], 2), to_near(down_two[half:], 1)]
    down_both = jnp.concatenate(far, axis=0)
    return (
        (gate, gate_one, gate_two, gate_both),
        (up, up_one, up_two, up_both),
        (down, down_one, down_two, down_both),
    )


def blocks_dot(rows, weights, block):
    return sum(
        jnp.dot(
            rows[:, place * block : (place + 1) * block], weight, preferred_element_type=jnp.float32
        )
        for place, weight in enumerate(weights)
    )


def plain_body(
    resid,
    queries,
    latent,
    rope_key,
    lat_gain,
    kv_weight,
    out_gain,
    out_weight,
    ffn_gain,
    gate_weight,
    up_weight,
    down_weight,
):
    gate_blocks, up_blocks, down_blocks = near_weights(gate_weight, up_weight, down_weight)
    rows_here = resid.shape[0]
    first_row = lax.axis_index("sp") * rows_here
    heads_here = queries.shape[1] // (NOPE + ROPE)
    columns = lax.axis_size("tp")
    column = lax.axis_index("tp")
    share = rows_here // columns
    query = jnp.concatenate(reorder(jnp.split(queries, columns, axis=0), column), axis=0)
    query = query.reshape(rows_here, heads_here, NOPE + ROPE)
    within = jnp.arange(rows_here, dtype=jnp.int32)
    own_columns = (within // share) ^ column
    query_index = first_row + own_columns * share + within % share
    query_nope = query[:, :, :NOPE]
    query_rope = rotate(
        query[:, :, NOPE:].astype(jnp.float32), query_index.astype(jnp.float32)[:, None]
    ).astype(jnp.bfloat16)
    scale = 1.0 / math.sqrt(NOPE + ROPE)

    def accumulate(state, key_value, key_rope):
        running_max, running_sum, weighted = state
        length = key_value.shape[0]
        key_value = key_value.reshape(length, heads_here, NOPE + VDIM)
        scores = jnp.einsum(
            "qhd,khd->hqk", query_nope, key_value[:, :, :NOPE], preferred_element_type=jnp.float32
        )
        scores = (
            scores
            + jnp.einsum("qhr,kr->hqk", query_rope, key_rope, preferred_element_type=jnp.float32)
        ) * scale
        allowed = (key_index[None, :] <= query_index[:, None])[None]
        scores = jnp.where(allowed, scores, LOWEST)
        new_max = jnp.maximum(running_max, jnp.max(scores, axis=-1))
        weights = jnp.where(allowed, jnp.exp(scores - new_max[:, :, None]), 0.0)
        running_sum = jnp.sum(weights, axis=-1)
        added = jnp.einsum(
            "hqk,khd->qhd",
            weights.astype(jnp.bfloat16),
            key_value[:, :, NOPE:],
            preferred_element_type=jnp.float32,
        )
        weighted = added
        return (new_max, running_sum, weighted)

    initial = (
        jnp.full((heads_here, rows_here), LOWEST, jnp.float32),
        jnp.zeros((heads_here, rows_here), jnp.float32),
        jnp.zeros((rows_here, heads_here, VDIM), jnp.float32),
    )
    ranks = lax.axis_size("sp")
    rank = lax.axis_index("sp")
    both = jnp.concatenate([latent, rope_key], axis=1)
    both = lax.dynamic_slice_in_dim(both, column * share, share, 0)
    pieces = [both]
    for step in range(1, ranks):
        onward = [(source, source + step) for source in range(ranks - step)]
        pieces.append(lax.ppermute(both, "sp", onward))
    both = gather_columns(jnp.concatenate(pieces, axis=0))
    within = jnp.arange(both.shape[0], dtype=jnp.int32)
    source = (rank - within // share % ranks + ranks) % ranks
    key_index = source * rows_here + ((within // (share * ranks)) ^ column) * share + within % share
    pieces = (both[:, : latent.shape[1]], both[:, latent.shape[1] :])

    def update(state):
        key_value, key_rope = make_keys(pieces[0], pieces[1], lat_gain, kv_weight, key_index)
        return accumulate(state, key_value, key_rope)

    _, running_sum, weighted = update(initial)
    attended = (weighted / jnp.transpose(running_sum)[:, :, None]).astype(jnp.bfloat16)
    attended_float = attended.reshape(rows_here, heads_here * VDIM).astype(jnp.float32)
    squares = jnp.split(jnp.sum(attended_float * attended_float, axis=1), columns)
    squares = lax.psum(jnp.concatenate(reorder(squares, column)), "tp")
    squares = jnp.concatenate(reorder(jnp.split(squares, columns), column))
    normed_out = attended_float * lax.rsqrt(squares / (HEADS * VDIM) + EPSILON)[:, None] * out_gain
    normed_out = normed_out.astype(jnp.bfloat16)
    own_first = lax.axis_index("tp") * share
    projected = jnp.dot(normed_out, out_weight, preferred_element_type=jnp.float32)
    projected = projected.astype(jnp.bfloat16)
    attn_sum = scatter_columns(projected).astype(jnp.float32)
    own_resid = lax.dynamic_slice_in_dim(resid, own_first, share, 0)
    middle = (own_resid.astype(jnp.float32) + attn_sum).astype(jnp.bfloat16)
    highs = ranks // GROUP
    high = rank // GROUP
    place = rank % GROUP
    width = resid.shape[1]
    block = width // ranks
    wide = GROUP * block
    mids = norm_rows(middle, ffn_gain).astype(jnp.bfloat16)
    mids = [
        to_high(
            by_distance(
                lax.dynamic_slice_in_dim(mids, (high + step) % highs * wide, wide, 1), place
            ),
            step,
            ranks,
        )
        for step in range(highs)
    ]
    mids = [gather_columns(piece) for piece in mids]
    gates, ups = None, None
    for step in list(range(1, highs)) + [0]:
        piece = mids[step]
        gate = blocks_dot(piece, gate_blocks, block)
        up = blocks_dot(piece, up_blocks, block)
        if step:
            gate = to_high(gate.astype(jnp.bfloat16), highs - step, ranks).astype(jnp.float32)
            up = to_high(up.astype(jnp.bfloat16), highs - step, ranks).astype(jnp.float32)
        gates = gate if gates is None else gates + gate
        ups = up if ups is None else ups + up
    hidden = (jax.nn.silu(gates) * ups).astype(jnp.bfloat16)
    received = [to_high(hidden, step, ranks) for step in range(highs)]
    terms = []
    for step in range(highs):
        partial = jnp.concatenate(
            [
                jnp.dot(received[step], weight, preferred_element_type=jnp.float32).astype(
                    jnp.bfloat16
                )
                for weight in down_blocks
            ],
            axis=1,
        )
        partial = to_high(scatter_columns(partial), highs - step, ranks)
        terms.append(by_distance(partial, place))
    terms = jnp.concatenate(terms, axis=1)
    ffn_sum = jnp.concatenate(
        [
            lax.dynamic_slice_in_dim(terms, (index - high + highs) % highs * wide, wide, 1)
            for index in range(highs)
        ],
        axis=1,
    ).astype(jnp.float32)
    return (middle.astype(jnp.float32) + ffn_sum).astype(jnp.bfloat16)


LANES = 128
PAIR = 2
LINE = 4
COLUMNS = 4
MESH = pl.DeviceIdType.MESH


ROW_ORDER = (1, 2, 0, 3)


def whole_step(
    query_ref,
    latent_ref,
    rope_ref,
    table_ref,
    lat_gain_ref,
    out_gain_ref,
    ffn_gain_ref,
    resid_hbm,
    kv_hbm,
    out_hbm,
    gate_hbm,
    up_hbm,
    down_hbm,
    result_ref,
    lat_mine,
    lat_buf,
    query,
    resid,
    kv_w,
    out_w,
    gate_up,
    down,
    act,
    hidden,
    top,
    norm,
    acc,
    stats_mine,
    stats_in,
    partial,
    core_in,
    near_out,
    near_in,
    partial_rows,
    core_rows,
    near_rows_out,
    near_rows_in,
    rows_out,
    rows_in,
    middle,
    total,
    local_sem,
    lat_send,
    lat_recv,
    lat_spread_send,
    lat_spread_recv,
    turn_send,
    turn_recv,
    pair_send,
    pair_recv,
    down_send,
    down_recv,
    act_line_send,
    act_line_recv,
    act_spread_send,
    act_spread_recv,
    stat_send,
    stat_recv,
    core_send,
    core_recv,
    near_send,
    near_recv,
    hid_send,
    hid_pass_send,
    hid_recv,
    core_rows_send,
    core_rows_recv,
    near_rows_send,
    near_rows_recv,
    rows_send,
    rows_recv,
):
    rank = lax.axis_index("sp")
    col = lax.axis_index("tp")
    ranks = lat_buf.shape[0]
    rows = lat_buf.shape[1]
    share = lat_mine.shape[0]
    width = resid.shape[1]
    units = hidden.shape[1] // LINE
    block = gate_hbm.shape[0]
    latent = kv_w.shape[0]
    heads = query.shape[0]
    z = rank // PAIR
    x = rank % PAIR
    mate = z * PAIR + (PAIR - 1 - x)
    inner = ((z + 1) // 2) % 2
    z_flips = [z, z + 1 - 2 * (z % 2), (z + 2) % LINE, LINE - 1 - z]
    col_flips = [col, col + 1 - 2 * (col % 2), (col + 2) % COLUMNS, COLUMNS - 1 - col]
    pending = []

    def remote(src, dst, send, recv, sp=None, tp=None):
        target = (rank if sp is None else sp, col if tp is None else tp)
        return pltpu.make_async_remote_copy(
            src_ref=src, dst_ref=dst, send_sem=send, recv_sem=recv, device_id=target,
            device_id_type=MESH,
        )

    def arrived(dst, recv):
        remote(dst, dst, recv, recv, tp=col_flips[1]).wait_recv()

    def send(copy, when=None):
        if when is None:
            copy.start()
        else:
            pl.when(when)(copy.start)
        pending.append((copy, when))

    def local(src, dst, slot):
        copy = pltpu.make_async_copy(src, dst, local_sem.at[slot])
        copy.start()
        return copy

    own_rows = pl.ds(pl.multiple_of(col * share, share), share)
    kv_copy = local(kv_hbm, kv_w, 0)
    out_copy = local(out_hbm, out_w, 1)
    resid_copy = local(resid_hbm.at[own_rows, :], resid, 2)

    def turned(values, cosine, sine):
        half = values.shape[1] // 2
        swapped = jnp.concatenate([values[:, half:], values[:, :half]], axis=1)
        return values * cosine + swapped * sine

    wide = latent_ref[own_rows, :].astype(jnp.float32)
    wide = wide * lax.rsqrt(jnp.mean(wide * wide, axis=1, keepdims=True) + EPSILON)
    lat_mine[:, :latent] = (wide * lat_gain_ref[...]).astype(jnp.bfloat16)
    key_rope = turned(
        rope_ref[own_rows, :].astype(jnp.float32), table_ref[own_rows, :ROPE],
        table_ref[own_rows, ROPE:],
    ).astype(jnp.bfloat16)
    lat_mine[:, latent:] = jnp.concatenate([key_rope, jnp.zeros_like(key_rope)], axis=1)

    barrier = pltpu.get_barrier_semaphore()
    for step in range(1, ranks):
        pl.semaphore_signal(
            barrier, inc=1, device_id=((rank + step) % ranks, col), device_id_type=MESH
        )
    for flip in col_flips[1:]:
        pl.semaphore_signal(barrier, inc=1, device_id=(rank, flip), device_id_type=MESH)
    pl.semaphore_wait(barrier, ranks - 1 + COLUMNS - 1)

    def lat_piece(source, column):
        return lat_buf.at[source, pl.ds(pl.multiple_of(column * share, share), share), :]

    def lat_spread(source, piece, flip, slot):
        return remote(
            piece, lat_piece(source, col_flips[slot - flip]),
            lat_spread_send.at[source, slot - 1], lat_spread_recv.at[source, slot - 1],
            tp=col_flips[flip],
        )

    for step in range(1, ranks):
        send(
            remote(
                lat_mine, lat_piece(rank, col), lat_send.at[step - 1], lat_recv.at[rank],
                sp=(rank + step) % ranks,
            ),
            rank + step < ranks,
        )
    lat_spread(rank, lat_mine, 2, 2).start()
    lat_spread(rank, lat_mine, 1, 1).start()
    lat_buf[rank, own_rows, :] = lat_mine[...]

    def region(kind, source):
        at = pl.multiple_of(source * block, block)
        return gate_up.at[pl.ds(at, block), pl.ds(kind * units, units)]

    def own_part(kind, place):
        at = pl.multiple_of(place * units, units)
        return (gate_hbm, up_hbm)[kind].at[:, pl.ds(at, units)]

    def down_part(half):
        middle_row = down_hbm.shape[0] // 2
        return pl.ds(half * middle_row, middle_row)

    def turn(kind):
        for k in range(1, LINE):
            send(
                remote(
                    own_part(kind, z_flips[k]), region(kind, rank), turn_send.at[kind, k],
                    turn_recv.at[kind, k], sp=z_flips[k] * PAIR + x,
                )
            )

    def pump(kind, k):
        here = region(kind, z_flips[k] * PAIR + x)
        if k:
            arrived(here, turn_recv.at[kind, k])
        send(
            remote(
                here if k else own_part(kind, z), here, pair_send.at[kind, k],
                pair_recv.at[kind, k], sp=mate,
            )
        )

    def paired(kind):
        for k in range(LINE):
            arrived(region(kind, z_flips[k] * PAIR + (PAIR - 1 - x)), pair_recv.at[kind, k])

    down_own = pl.ds(pl.multiple_of(x * down_hbm.shape[1], LANES), down_hbm.shape[1])
    down_mate = pl.ds(
        pl.multiple_of((PAIR - 1 - x) * down_hbm.shape[1], LANES), down_hbm.shape[1]
    )

    def pump_down(half):
        send(
            remote(
                down_hbm.at[down_part(half), :], down.at[down_part(half), down_own],
                down_send.at[half], down_recv.at[half], sp=mate,
            )
        )

    turn(0)
    turn(1)
    pump(0, 0)
    pump(1, 0)
    pump_down(0)
    own_copies = [local(own_part(kind, z), region(kind, rank), 3 + kind) for kind in range(2)]
    own_copies.append(local(down_hbm, down.at[:, down_own], 5))

    for head in range(heads):
        at = head * (NOPE + ROPE)
        rotary = turned(
            query_ref[:, at + NOPE : at + NOPE + ROPE].astype(jnp.float32), table_ref[:, :ROPE],
            table_ref[:, ROPE:],
        ).astype(jnp.bfloat16)
        query[head, :, :NOPE] = query_ref[:, at : at + NOPE]
        query[head, :, NOPE:] = jnp.concatenate([rotary, jnp.zeros_like(rotary)], axis=1)
    top[...] = jnp.full(top.shape, LOWEST, jnp.float32)
    norm[...] = jnp.zeros(norm.shape, jnp.float32)
    acc[...] = jnp.zeros(acc.shape, jnp.float32)
    scale = math.log2(math.e) / math.sqrt(NOPE + ROPE)
    kv_copy.wait()

    def attend(index, carry):
        source = rank - index

        @pl.when(index < rank)
        def _():
            arrived(lat_piece(source - 1, col), lat_recv.at[source - 1])
            piece = lat_piece(source - 1, col)
            lat_spread(source - 1, piece, 2, 2).start()
            lat_spread(source - 1, piece, 1, 1).start()

        arrived(lat_piece(source, col_flips[2]), lat_spread_recv.at[source, 1])
        lat_spread(source, lat_piece(source, col_flips[2]), 1, 3).start()
        arrived(lat_piece(source, col_flips[1]), lat_spread_recv.at[source, 0])
        arrived(lat_piece(source, col_flips[3]), lat_spread_recv.at[source, 2])
        key_value = jnp.dot(
            lat_buf[source, :, :latent], kv_w[...], preferred_element_type=jnp.float32
        ).astype(jnp.bfloat16)
        key_rope = lat_buf[source, :, latent:]
        row_of = lax.broadcasted_iota(jnp.int32, (rows, rows), 0) + index * rows
        allowed = lax.broadcasted_iota(jnp.int32, (rows, rows), 1) <= row_of
        for head in range(heads):
            at = head * (NOPE + VDIM)
            keys = jnp.concatenate([key_value[:, at : at + NOPE], key_rope], axis=1)
            scores = lax.dot_general(
                query[head], keys, (((1,), (1,)), ((), ())), preferred_element_type=jnp.float32
            )
            scores = jnp.where(allowed, scores * scale, LOWEST)
            old = top[head]
            new = jnp.maximum(old, jnp.max(scores, axis=1, keepdims=True))
            weights = jnp.exp2(scores - new[:, :1])
            fade = jnp.exp2(old - new)
            top[head] = new
            norm[head] = norm[head] * fade + jnp.sum(weights, axis=1, keepdims=True)
            across = slice(head * VDIM, (head + 1) * VDIM)
            acc[:, across] = acc[:, across] * fade + jnp.dot(
                weights.astype(jnp.bfloat16), key_value[:, at + NOPE : at + NOPE + VDIM],
                preferred_element_type=jnp.float32,
            )
        return carry

    lax.fori_loop(0, rank + 1, attend, 0)

    squares = jnp.zeros((rows, 1), jnp.float32)
    attended = []
    for head in range(heads):
        across = slice(head * VDIM, (head + 1) * VDIM)
        part = (acc[:, across] / norm[head]).astype(jnp.bfloat16).astype(jnp.float32)
        squares = squares + jnp.sum(part * part, axis=1, keepdims=True)
        attended.append((part * out_gain_ref[:, across]).astype(jnp.bfloat16))
    attended = jnp.concatenate(attended, axis=1)
    stats_mine[...] = jnp.broadcast_to(squares, stats_mine.shape)

    chunk = 4 * LANES

    def piece_of(ref, column):
        return ref.at[pl.ds(pl.multiple_of(column * share, share), share), :]

    def project(left, right, target):
        def one(index, carry):
            at = pl.ds(pl.multiple_of(index * chunk, chunk), chunk)
            target[:, at] = jnp.dot(
                left, right[:, at], preferred_element_type=jnp.float32
            ).astype(jnp.bfloat16)
            return carry

        lax.fori_loop(0, right.shape[1] // chunk, one, 0)

    def each_chunk(across, work):
        def one(index, carry):
            work(pl.ds(pl.multiple_of(index * chunk, chunk), chunk))
            return carry

        lax.fori_loop(0, across // chunk, one, 0)

    def fold(part, core, out, near, sems):
        core_s, core_r, near_s, near_r = sems
        for slot, column in ((1, 3), (0, 1)):
            send(
                remote(
                    piece_of(part, col_flips[column]), core.at[slot], core_s.at[slot],
                    core_r.at[slot], tp=col_flips[1],
                )
            )
        arrived(core.at[1], core_r.at[1])
        theirs = pl.ds(pl.multiple_of(col_flips[2] * share, share), share)

        def add(at):
            out[:, at] = (
                part[theirs, at].astype(jnp.float32) + core[1, :, at].astype(jnp.float32)
            ).astype(jnp.bfloat16)

        each_chunk(out.shape[1], add)
        send(remote(out, near, near_s, near_r, tp=col_flips[2]))
        arrived(core.at[0], core_r.at[0])

    def folded(part, core, near, sems, keep):
        arrived(near, sems[3])

        def add(at):
            keep(
                at,
                part[own_rows, at].astype(jnp.float32)
                + core[0, :, at].astype(jnp.float32)
                + near[:, at].astype(jnp.float32),
            )

        each_chunk(near.shape[1], add)

    out_copy.wait()
    for m in range(1, COLUMNS):
        send(
            remote(
                stats_mine.at[pl.ds(pl.multiple_of(col_flips[m] * share, share), share), :],
                stats_in.at[m - 1], stat_send.at[m - 1], stat_recv.at[m - 1], tp=col_flips[m],
            )
        )
    project(attended, out_w, partial)
    first = (core_send, core_recv, near_send.at[0], near_recv.at[0])
    fold(partial, core_in, near_out, near_in, first)
    for k in range(1, LINE):
        pump(0, k)
    squares = stats_mine[own_rows, :]
    for m in range(1, COLUMNS):
        arrived(stats_in.at[m - 1], stat_recv.at[m - 1])
        squares = squares + stats_in[m - 1]
    factor = lax.rsqrt(squares / (HEADS * VDIM) + EPSILON)[:, :1]

    def keep_total(at, values):
        total[:, at] = values

    folded(partial, core_in, near_in, first, keep_total)
    resid_copy.wait()
    squares = jnp.zeros((share, 1), jnp.float32)
    for index in range(width // chunk):
        at = slice(index * chunk, (index + 1) * chunk)
        mid = (resid[:, at].astype(jnp.float32) + total[:, at] * factor).astype(jnp.bfloat16)
        middle[:, at] = mid
        mid = mid.astype(jnp.float32)
        squares = squares + jnp.sum(mid * mid, axis=1, keepdims=True)
    factor = lax.rsqrt(squares / width + EPSILON)

    def act_piece(place, column):
        at = pl.multiple_of(place * rows + column * share, share)
        return act.at[pl.ds(at, share), :]

    at_own = pl.ds(pl.multiple_of(z * rows + col * share, share), share)
    for index in range(width // chunk):
        at = slice(index * chunk, (index + 1) * chunk)
        act[at_own, at] = (
            middle[:, at].astype(jnp.float32) * factor * ffn_gain_ref[:, at]
        ).astype(jnp.bfloat16)

    def up_line(src, dst, send_sem, recv_sem, when):
        send(remote(src, dst, send_sem, recv_sem, sp=(rank + PAIR) % ranks), when)

    def down_line(src, dst, send_sem, recv_sem, when):
        send(remote(src, dst, send_sem, recv_sem, sp=(rank + ranks - PAIR) % ranks), when)

    def act_spread(place, flip, slot):
        piece = act_piece(place, col_flips[slot - flip])
        send(
            remote(
                piece, piece, act_spread_send.at[place, slot - 1],
                act_spread_recv.at[place, slot - 1], tp=col_flips[flip],
            )
        )

    mine = act_piece(z, col)
    up_line(mine, mine, act_line_send.at[0], act_line_recv.at[z], z < LINE - 1)
    down_line(mine, mine, act_line_send.at[1], act_line_recv.at[z], z > 0)
    act_spread(z, 2, 2)
    act_spread(z, 1, 1)
    order = [
        z,
        z_flips[1],
        z_flips[2] * (1 - inner) + z_flips[3] * inner,
        z_flips[3] * (1 - inner) + z_flips[2] * inner,
    ]

    def near_act(place):
        arrived(act_piece(place, col_flips[2]), act_spread_recv.at[place, 1])
        act_spread(place, 1, 3)

    for index in range(1, LINE):
        nearer = order[index]
        piece = act_piece(nearer, col)
        arrived(piece, act_line_recv.at[nearer])
        up_line(
            piece, piece, act_line_send.at[2 * index], act_line_recv.at[nearer],
            (nearer < z) & (z < LINE - 1),
        )
        down_line(
            piece, piece, act_line_send.at[2 * index + 1], act_line_recv.at[nearer],
            (nearer > z) & (z > 0),
        )
        act_spread(nearer, 2, 2)
        act_spread(nearer, 1, 1)
        near_act(order[index - 1])
        if index == 1:
            pump(1, 1)
        elif index == 2:
            pump(1, 2)
            pump(1, 3)
            pump_down(1)

    for copy in own_copies:
        copy.wait()
    paired(0)
    paired(1)

    def hid_piece(place, source):
        return hidden.at[
            pl.ds(place * rows, rows), pl.ds(pl.multiple_of(source * units, units), units)
        ]

    def gated(index):
        place = ROW_ORDER[index]
        arrived(act_piece(place, col_flips[1]), act_spread_recv.at[place, 0])
        arrived(act_piece(place, col_flips[3]), act_spread_recv.at[place, 2])
        here = slice(place * rows, (place + 1) * rows)
        both = jnp.dot(act[here, :], gate_up[...], preferred_element_type=jnp.float32)
        gate = both[:, :units]
        hidden[here, pl.ds(pl.multiple_of(z * units, units), units)] = (
            gate / (1.0 + jnp.exp(-gate)) * both[:, units:]
        ).astype(jnp.bfloat16)
        piece = hid_piece(place, z)
        up_line(piece, piece, hid_send.at[index, 0], hid_recv.at[place, z], z < LINE - 1)
        down_line(piece, piece, hid_send.at[index, 1], hid_recv.at[place, z], z > 0)

    def pass_hidden(index, distance):
        place = ROW_ORDER[index]
        for side, source, when in (
            (0, z - distance, (z - distance >= 0) & (z < LINE - 1)),
            (1, z + distance, (z + distance < LINE) & (z > 0)),
        ):
            source = (source + LINE) % LINE
            piece = hid_piece(place, source)
            copy = remote(
                piece, piece, hid_pass_send.at[index, distance - 1, side],
                hid_recv.at[place, source],
                sp=((rank + PAIR) if side == 0 else (rank + ranks - PAIR)) % ranks,
            )

            @pl.when(when)
            def _():
                arrived(piece, hid_recv.at[place, source])
                copy.start()

            pending.append((copy, when))

    def hidden_all(index):
        place = ROW_ORDER[index]
        for distance in range(1, LINE):
            for source, when in (
                (LINE - 1 - distance, z == LINE - 1),
                (distance, z == 0),
            ):

                @pl.when(when)
                def _():
                    arrived(hid_piece(place, source), hid_recv.at[place, source])

    def row_sems(index):
        return (
            core_rows_send.at[index], core_rows_recv.at[index], near_rows_send.at[index],
            near_rows_recv.at[index],
        )

    def start_rows(index):
        place = ROW_ORDER[index]
        hidden_all(index)
        project(hidden[place * rows : (place + 1) * rows, :], down, partial_rows.at[index])
        fold(
            partial_rows.at[index], core_rows.at[index], near_rows_out.at[index],
            near_rows_in.at[index], row_sems(index),
        )

    def end_rows(index):
        place = ROW_ORDER[index]

        def keep(at, values):
            rows_out[index, :, at] = values.astype(jnp.bfloat16)

        folded(
            partial_rows.at[index], core_rows.at[index], near_rows_in.at[index], row_sems(index),
            keep,
        )
        send(
            remote(
                rows_out.at[index], rows_in.at[z], rows_send.at[index], rows_recv.at[z],
                sp=place * PAIR + x,
            ),
            z != place,
        )

        @pl.when(z == place)
        def _():
            rows_in[z] = rows_out[index]


    gated(0)
    gated(1)
    near_act(order[LINE - 1])
    pass_hidden(0, 1)
    gated(2)
    pass_hidden(1, 1)
    pass_hidden(0, 2)
    gated(3)
    pass_hidden(2, 1)
    pass_hidden(1, 2)
    for half in range(2):
        arrived(down.at[down_part(half), down_mate], down_recv.at[half])
    start_rows(0)
    pass_hidden(3, 1)
    pass_hidden(2, 2)
    start_rows(1)
    end_rows(0)
    pass_hidden(3, 2)
    start_rows(2)
    end_rows(1)
    start_rows(3)
    end_rows(2)
    end_rows(3)
    for source in range(LINE):

        @pl.when(z != source)
        def _():
            arrived(rows_in.at[source], rows_recv.at[source])

    part = rows_in.shape[2]
    for source in range(LINE):
        at = slice(source * part, (source + 1) * part)
        result_ref[:, at] = (
            middle[:, at].astype(jnp.float32) + rows_in[source].astype(jnp.float32)
        ).astype(jnp.bfloat16)

    for copy, when in pending:
        if when is None:
            copy.wait_send()
        else:
            pl.when(when)(copy.wait_send)

    def drain(source, carry):
        piece = lat_piece(source, col)
        for slot in range(COLUMNS - 1):
            remote(
                piece, piece, lat_spread_send.at[source, slot], lat_spread_send.at[source, slot],
                tp=col_flips[1],
            ).wait_send()
        return carry

    lax.fori_loop(0, rank + 1, drain, 0)


def fused_body(
    resid,
    queries,
    latent,
    rope_key,
    lat_gain,
    kv_weight,
    out_gain,
    out_weight,
    ffn_gain,
    gate_weight,
    up_weight,
    down_weight,
):
    ranks, columns = lax.axis_size("sp"), lax.axis_size("tp")
    rank = lax.axis_index("sp")
    rows, width = resid.shape
    share = rows // columns
    heads = queries.shape[1] // (NOPE + ROPE)
    units = gate_weight.shape[1] // LINE
    block = gate_weight.shape[0]
    depth = latent.shape[1]
    places = (rank * rows + jnp.arange(rows, dtype=jnp.int32)).astype(jnp.float32)
    half = ROPE // 2
    inverse = THETA ** (-jnp.arange(half, dtype=jnp.float32) / half)
    angle = places[:, None] * inverse
    cosine, sine = jnp.cos(angle), jnp.sin(angle)
    table = jnp.concatenate([cosine, cosine, -sine, sine], axis=1)
    bf, f32 = jnp.bfloat16, jnp.float32
    dma = pltpu.SemaphoreType.DMA
    vmem = pl.BlockSpec(memory_space=pltpu.VMEM)
    anywhere = pl.BlockSpec(memory_space=pl.ANY)
    part = width // LINE
    others = columns - 1
    return pl.pallas_call(
        whole_step,
        out_shape=jax.ShapeDtypeStruct((share, width), bf),
        in_specs=[vmem] * 7 + [anywhere] * 6,
        out_specs=vmem,
        scratch_shapes=[
            pltpu.VMEM((share, depth + LANES), bf),
            pltpu.VMEM((ranks, rows, depth + LANES), bf),
            pltpu.VMEM((heads, rows, 2 * LANES), bf),
            pltpu.VMEM((share, width), bf),
            pltpu.VMEM(kv_weight.shape, bf),
            pltpu.VMEM(out_weight.shape, bf),
            pltpu.VMEM((ranks * block, 2 * units), bf),
            pltpu.VMEM((LINE * units, PAIR * down_weight.shape[1]), bf),
            pltpu.VMEM((LINE * rows, width), bf),
            pltpu.VMEM((LINE * rows, LINE * units), bf),
            pltpu.VMEM((heads, rows, LANES), f32),
            pltpu.VMEM((heads, rows, LANES), f32),
            pltpu.VMEM((rows, heads * VDIM), f32),
            pltpu.VMEM((rows, LANES), f32),
            pltpu.VMEM((others, share, LANES), f32),
            pltpu.VMEM((rows, width), bf),
            pltpu.VMEM((2, share, width), bf),
            pltpu.VMEM((share, width), bf),
            pltpu.VMEM((share, width), bf),
            pltpu.VMEM((LINE, rows, part), bf),
            pltpu.VMEM((LINE, 2, share, part), bf),
            pltpu.VMEM((LINE, share, part), bf),
            pltpu.VMEM((LINE, share, part), bf),
            pltpu.VMEM((LINE, share, part), bf),
            pltpu.VMEM((LINE, share, part), bf),
            pltpu.VMEM((share, width), bf),
            pltpu.VMEM((share, width), f32),
            dma((6,)),
            dma((ranks - 1,)),
            dma((ranks,)),
            dma((ranks, others)),
            dma((ranks, others)),
            dma((2, LINE)),
            dma((2, LINE)),
            dma((2, LINE)),
            dma((2, LINE)),
            dma((2,)),
            dma((2,)),
            dma((2 * LINE,)),
            dma((LINE,)),
            dma((LINE, others)),
            dma((LINE, others)),
            dma((others,)),
            dma((others,)),
            dma((2,)),
            dma((2,)),
            dma((1,)),
            dma((1,)),
            dma((LINE, 2)),
            dma((LINE, 2, 2)),
            dma((LINE, LINE)),
            dma((LINE, 2)),
            dma((LINE, 2)),
            dma((LINE,)),
            dma((LINE,)),
            dma((LINE,)),
            dma((LINE,)),
        ],
        compiler_params=pltpu.CompilerParams(
            collective_id=0, has_side_effects=True, vmem_limit_bytes=66 * 1024 * 1000
        ),
    )(
        queries,
        latent,
        rope_key,
        table,
        lat_gain.reshape(1, -1),
        out_gain.reshape(1, -1),
        ffn_gain.reshape(1, -1),
        resid,
        kv_weight,
        out_weight,
        gate_weight,
        up_weight,
        down_weight,
    )


def solution(mesh):
    placed = (
        P("sp", None),
        P("sp", "tp"),
        P("sp", None),
        P("sp", None),
        P(),
        P(None, "tp"),
        P("tp"),
        P("tp", None),
        P(),
        P("sp", "tp"),
        P("sp", "tp"),
        P("tp", "sp"),
    )

    def mapped(function):
        return jax.shard_map(
            function, mesh=mesh, in_specs=placed, out_specs=P(("sp", "tp"), None), check_vma=False
        )

    if mesh.shape["sp"] == PAIR * LINE and mesh.shape["tp"] == COLUMNS:
        return mapped(fused_body)
    return mapped(plain_body)
```

```python
import functools
import math

import jax
import jax.numpy as jnp
from jax import lax
from jax.experimental import pallas as pl
from jax.experimental.pallas import tpu as pltpu
from jax.sharding import PartitionSpec as P


HEADS = 16
NOPE = 128
ROPE = 64
VDIM = 128


EPSILON = 1e-06
THETA = 10000.0
LOWEST = -1e30
GROUP = 4


def rotate(values, places):
    half = values.shape[-1] // 2
    inverse = THETA ** (-jnp.arange(half, dtype=jnp.float32) / half)
    angle = places[..., None] * inverse
    cosine = jnp.cos(angle)
    sine = jnp.sin(angle)
    first = values[..., :half]
    second = values[..., half:]
    return jnp.concatenate(
        [first * cosine - second * sine, first * sine + second * cosine], axis=-1
    )


def norm_rows(values, gain):
    wide = values.astype(jnp.float32)
    return wide * lax.rsqrt(jnp.mean(wide * wide, axis=-1, keepdims=True) + EPSILON) * gain


def make_keys(latent_piece, rotary_piece, lat_gain, kv_weight, key_index):
    normed = norm_rows(latent_piece, lat_gain).astype(jnp.bfloat16)
    key_value = jnp.dot(normed, kv_weight, preferred_element_type=jnp.float32)
    key_value = key_value.astype(jnp.bfloat16)
    key_rope = rotate(rotary_piece.astype(jnp.float32), key_index.astype(jnp.float32)).astype(
        jnp.bfloat16
    )
    return (key_value, key_rope)


def to_near(values, flip):
    ranks = lax.axis_size("sp")
    return lax.ppermute(values, "sp", [(rank, rank ^ flip) for rank in range(ranks)])


def to_high(values, step, ranks):
    if step % (ranks // GROUP) == 0:
        return values
    return lax.ppermute(
        values, "sp", [(rank, (rank + step * GROUP) % ranks) for rank in range(ranks)]
    )


def reorder(blocks, place):
    bit = 1
    while bit < len(blocks):
        swap = place // bit % 2 == 1
        blocks = [jnp.where(swap, blocks[j ^ bit], blocks[j]) for j in range(len(blocks))]
        bit *= 2
    return blocks


def by_distance(values, place):
    return jnp.concatenate(reorder(jnp.split(values, GROUP, axis=1), place), axis=1)


def to_column(values, bit):
    columns = lax.axis_size("tp")
    return lax.ppermute(values, "tp", [(column, column ^ bit) for column in range(columns)])


def gather_columns(values):
    rows = values.shape[0]
    held = {0: values}
    bit = lax.axis_size("tp") // 2
    while bit:
        keys = sorted(held)
        theirs = to_column(jnp.concatenate([held[key] for key in keys], axis=0), bit)
        for at, key in enumerate(keys):
            held[key + bit] = theirs[at * rows : (at + 1) * rows]
        bit //= 2
    return jnp.concatenate([held[key] for key in sorted(held)], axis=0)


def scatter_columns(values):
    columns = lax.axis_size("tp")
    blocks = dict(enumerate(jnp.split(values, columns, axis=0)))
    bit = 1
    while bit < columns:
        mine = [key for key in sorted(blocks) if not key & bit]
        theirs = to_column(jnp.concatenate([blocks[key + bit] for key in mine], axis=0), bit)
        theirs = jnp.split(theirs, len(mine), axis=0)
        blocks = {
            key: (blocks[key].astype(jnp.float32) + piece.astype(jnp.float32)).astype(jnp.bfloat16)
            for key, piece in zip(mine, theirs)
        }
        bit *= 2
    return blocks[0]


def near_weights(gate, up, down):
    gate_one = to_near(gate, 1)
    up_two = to_near(up, 2)
    up_one = to_near(up, 1)
    gate_two = to_near(gate, 2)
    gate_both = to_near(gate_one, 2)
    up_both = to_near(up_two, 1)
    down, gate_both, up_both = lax.optimization_barrier((down, gate_both, up_both))
    half = down.shape[0] // 2
    down_one = to_near(down, 1)
    down_two = to_near(down, 2)
    far = [to_near(down_one[:half], 2), to_near(down_two[half:], 1)]
    down_both = jnp.concatenate(far, axis=0)
    return (
        (gate, gate_one, gate_two, gate_both),
        (up, up_one, up_two, up_both),
        (down, down_one, down_two, down_both),
    )


def blocks_dot(rows, weights, block):
    return sum(
        jnp.dot(
            rows[:, place * block : (place + 1) * block], weight, preferred_element_type=jnp.float32
        )
        for place, weight in enumerate(weights)
    )


def plain_body(
    resid,
    queries,
    latent,
    rope_key,
    lat_gain,
    kv_weight,
    out_gain,
    out_weight,
    ffn_gain,
    gate_weight,
    up_weight,
    down_weight,
):
    gate_blocks, up_blocks, down_blocks = near_weights(gate_weight, up_weight, down_weight)
    rows_here = resid.shape[0]
    first_row = lax.axis_index("sp") * rows_here
    heads_here = queries.shape[1] // (NOPE + ROPE)
    columns = lax.axis_size("tp")
    column = lax.axis_index("tp")
    share = rows_here // columns
    query = jnp.concatenate(reorder(jnp.split(queries, columns, axis=0), column), axis=0)
    query = query.reshape(rows_here, heads_here, NOPE + ROPE)
    within = jnp.arange(rows_here, dtype=jnp.int32)
    own_columns = (within // share) ^ column
    query_index = first_row + own_columns * share + within % share
    query_nope = query[:, :, :NOPE]
    query_rope = rotate(
        query[:, :, NOPE:].astype(jnp.float32), query_index.astype(jnp.float32)[:, None]
    ).astype(jnp.bfloat16)
    scale = 1.0 / math.sqrt(NOPE + ROPE)

    def accumulate(state, key_value, key_rope):
        running_max, running_sum, weighted = state
        length = key_value.shape[0]
        key_value = key_value.reshape(length, heads_here, NOPE + VDIM)
        scores = jnp.einsum(
            "qhd,khd->hqk", query_nope, key_value[:, :, :NOPE], preferred_element_type=jnp.float32
        )
        scores = (
            scores
            + jnp.einsum("qhr,kr->hqk", query_rope, key_rope, preferred_element_type=jnp.float32)
        ) * scale
        allowed = (key_index[None, :] <= query_index[:, None])[None]
        scores = jnp.where(allowed, scores, LOWEST)
        new_max = jnp.maximum(running_max, jnp.max(scores, axis=-1))
        weights = jnp.where(allowed, jnp.exp(scores - new_max[:, :, None]), 0.0)
        running_sum = jnp.sum(weights, axis=-1)
        added = jnp.einsum(
            "hqk,khd->qhd",
            weights.astype(jnp.bfloat16),
            key_value[:, :, NOPE:],
            preferred_element_type=jnp.float32,
        )
        weighted = added
        return (new_max, running_sum, weighted)

    initial = (
        jnp.full((heads_here, rows_here), LOWEST, jnp.float32),
        jnp.zeros((heads_here, rows_here), jnp.float32),
        jnp.zeros((rows_here, heads_here, VDIM), jnp.float32),
    )
    ranks = lax.axis_size("sp")
    rank = lax.axis_index("sp")
    both = jnp.concatenate([latent, rope_key], axis=1)
    both = lax.dynamic_slice_in_dim(both, column * share, share, 0)
    pieces = [both]
    for step in range(1, ranks):
        onward = [(source, source + step) for source in range(ranks - step)]
        pieces.append(lax.ppermute(both, "sp", onward))
    both = gather_columns(jnp.concatenate(pieces, axis=0))
    within = jnp.arange(both.shape[0], dtype=jnp.int32)
    source = (rank - within // share % ranks + ranks) % ranks
    key_index = source * rows_here + ((within // (share * ranks)) ^ column) * share + within % share
    pieces = (both[:, : latent.shape[1]], both[:, latent.shape[1] :])

    def update(state):
        key_value, key_rope = make_keys(pieces[0], pieces[1], lat_gain, kv_weight, key_index)
        return accumulate(state, key_value, key_rope)

    _, running_sum, weighted = update(initial)
    attended = (weighted / jnp.transpose(running_sum)[:, :, None]).astype(jnp.bfloat16)
    attended_float = attended.reshape(rows_here, heads_here * VDIM).astype(jnp.float32)
    squares = jnp.split(jnp.sum(attended_float * attended_float, axis=1), columns)
    squares = lax.psum(jnp.concatenate(reorder(squares, column)), "tp")
    squares = jnp.concatenate(reorder(jnp.split(squares, columns), column))
    normed_out = attended_float * lax.rsqrt(squares / (HEADS * VDIM) + EPSILON)[:, None] * out_gain
    normed_out = normed_out.astype(jnp.bfloat16)
    own_first = lax.axis_index("tp") * share
    projected = jnp.dot(normed_out, out_weight, preferred_element_type=jnp.float32)
    projected = projected.astype(jnp.bfloat16)
    attn_sum = scatter_columns(projected).astype(jnp.float32)
    own_resid = lax.dynamic_slice_in_dim(resid, own_first, share, 0)
    middle = (own_resid.astype(jnp.float32) + attn_sum).astype(jnp.bfloat16)
    highs = ranks // GROUP
    high = rank // GROUP
    place = rank % GROUP
    width = resid.shape[1]
    block = width // ranks
    wide = GROUP * block
    mids = norm_rows(middle, ffn_gain).astype(jnp.bfloat16)
    mids = [
        to_high(
            by_distance(
                lax.dynamic_slice_in_dim(mids, (high + step) % highs * wide, wide, 1), place
            ),
            step,
            ranks,
        )
        for step in range(highs)
    ]
    mids = [gather_columns(piece) for piece in mids]
    gates, ups = None, None
    for step in list(range(1, highs)) + [0]:
        piece = mids[step]
        gate = blocks_dot(piece, gate_blocks, block)
        up = blocks_dot(piece, up_blocks, block)
        if step:
            gate = to_high(gate.astype(jnp.bfloat16), highs - step, ranks).astype(jnp.float32)
            up = to_high(up.astype(jnp.bfloat16), highs - step, ranks).astype(jnp.float32)
        gates = gate if gates is None else gates + gate
        ups = up if ups is None else ups + up
    hidden = (jax.nn.silu(gates) * ups).astype(jnp.bfloat16)
    received = [to_high(hidden, step, ranks) for step in range(highs)]
    terms = []
    for step in range(highs):
        partial = jnp.concatenate(
            [
                jnp.dot(received[step], weight, preferred_element_type=jnp.float32).astype(
                    jnp.bfloat16
                )
                for weight in down_blocks
            ],
            axis=1,
        )
        partial = to_high(scatter_columns(partial), highs - step, ranks)
        terms.append(by_distance(partial, place))
    terms = jnp.concatenate(terms, axis=1)
    ffn_sum = jnp.concatenate(
        [
            lax.dynamic_slice_in_dim(terms, (index - high + highs) % highs * wide, wide, 1)
            for index in range(highs)
        ],
        axis=1,
    ).astype(jnp.float32)
    return (middle.astype(jnp.float32) + ffn_sum).astype(jnp.bfloat16)


LANES = 128
PAIR = 2
LINE = 4
COLUMNS = 4
MESH = pl.DeviceIdType.MESH


PARTS = 4


def whole_step(
    query_ref,
    latent_ref,
    rope_ref,
    table_ref,
    lat_gain_ref,
    out_gain_ref,
    ffn_gain_ref,
    resid_hbm,
    kv_hbm,
    out_hbm,
    gate_hbm,
    up_hbm,
    down_hbm,
    result_ref,
    lat_mine,
    lat_buf,
    query,
    resid,
    kv_w,
    out_w,
    gate_up,
    down,
    act,
    hidden,
    top,
    norm,
    acc,
    stats_mine,
    stats_in,
    partial,
    core_in,
    near_out,
    near_in,
    partial_rows,
    core_rows,
    near_rows_out,
    near_rows_in,
    rows_out,
    rows_in,
    middle,
    total,
    local_sem,
    lat_send,
    lat_recv,
    lat_spread_send,
    lat_spread_recv,
    turn_send,
    turn_recv,
    pair_send,
    pair_recv,
    down_send,
    down_recv,
    act_line_send,
    act_line_recv,
    act_spread_send,
    act_spread_recv,
    stat_send,
    stat_recv,
    core_send,
    core_recv,
    near_send,
    near_recv,
    hid_send,
    hid_pass_send,
    hid_recv,
    core_rows_send,
    core_rows_recv,
    near_rows_send,
    near_rows_recv,
    rows_send,
    rows_recv,
):
    rank = lax.axis_index("sp")
    col = lax.axis_index("tp")
    ranks = lat_buf.shape[0]
    rows = lat_buf.shape[1]
    share = lat_mine.shape[0]
    width = resid.shape[1]
    units = hidden.shape[1] // LINE
    block = gate_hbm.shape[0]
    latent = kv_w.shape[0]
    heads = query.shape[0]
    z = rank // PAIR
    x = rank % PAIR
    mate = z * PAIR + (PAIR - 1 - x)
    inner = ((z + 1) // 2) % 2
    z_flips = [z, z + 1 - 2 * (z % 2), (z + 2) % LINE, LINE - 1 - z]
    col_flips = [col, col + 1 - 2 * (col % 2), (col + 2) % COLUMNS, COLUMNS - 1 - col]
    pending = []

    def remote(src, dst, send, recv, sp=None, tp=None):
        target = (rank if sp is None else sp, col if tp is None else tp)
        return pltpu.make_async_remote_copy(
            src_ref=src, dst_ref=dst, send_sem=send, recv_sem=recv, device_id=target,
            device_id_type=MESH,
        )

    def arrived(dst, recv):
        remote(dst, dst, recv, recv, tp=col_flips[1]).wait_recv()

    def send(copy, when=None):
        if when is None:
            copy.start()
        else:
            pl.when(when)(copy.start)
        pending.append((copy, when))

    def local(src, dst, slot):
        copy = pltpu.make_async_copy(src, dst, local_sem.at[slot])
        copy.start()
        return copy

    own_rows = pl.ds(pl.multiple_of(col * share, share), share)
    kv_copy = local(kv_hbm, kv_w, 0)
    out_copy = local(out_hbm, out_w, 1)
    resid_copy = local(resid_hbm.at[own_rows, :], resid, 2)

    def turned(values, cosine, sine):
        half = values.shape[1] // 2
        swapped = jnp.concatenate([values[:, half:], values[:, :half]], axis=1)
        return values * cosine + swapped * sine

    wide = latent_ref[own_rows, :].astype(jnp.float32)
    wide = wide * lax.rsqrt(jnp.mean(wide * wide, axis=1, keepdims=True) + EPSILON)
    lat_mine[:, :latent] = (wide * lat_gain_ref[...]).astype(jnp.bfloat16)
    key_rope = turned(
        rope_ref[own_rows, :].astype(jnp.float32), table_ref[own_rows, :ROPE],
        table_ref[own_rows, ROPE:],
    ).astype(jnp.bfloat16)
    lat_mine[:, latent:] = jnp.concatenate([key_rope, jnp.zeros_like(key_rope)], axis=1)

    barrier = pltpu.get_barrier_semaphore()
    for step in range(1, ranks):
        pl.semaphore_signal(
            barrier, inc=1, device_id=((rank + step) % ranks, col), device_id_type=MESH
        )
    for flip in col_flips[1:]:
        pl.semaphore_signal(barrier, inc=1, device_id=(rank, flip), device_id_type=MESH)
    pl.semaphore_wait(barrier, ranks - 1 + COLUMNS - 1)

    def lat_piece(source, column):
        return lat_buf.at[source, pl.ds(pl.multiple_of(column * share, share), share), :]

    def lat_spread(source, piece, flip, slot):
        return remote(
            piece, lat_piece(source, col_flips[slot - flip]),
            lat_spread_send.at[source, slot - 1], lat_spread_recv.at[source, slot - 1],
            tp=col_flips[flip],
        )

    for step in range(1, ranks):
        send(
            remote(
                lat_mine, lat_piece(rank, col), lat_send.at[step - 1], lat_recv.at[rank],
                sp=(rank + step) % ranks,
            ),
            rank + step < ranks,
        )
    lat_spread(rank, lat_mine, 2, 2).start()
    lat_spread(rank, lat_mine, 1, 1).start()
    lat_buf[rank, own_rows, :] = lat_mine[...]

    def region(kind, source):
        at = pl.multiple_of(source * block, block)
        return gate_up.at[pl.ds(at, block), pl.ds(kind * units, units)]

    def own_part(kind, place):
        at = pl.multiple_of(place * units, units)
        return (gate_hbm, up_hbm)[kind].at[:, pl.ds(at, units)]

    def down_part(half):
        middle_row = down_hbm.shape[0] // 2
        return pl.ds(half * middle_row, middle_row)

    def turn(kind):
        for k in range(1, LINE):
            send(
                remote(
                    own_part(kind, z_flips[k]), region(kind, rank), turn_send.at[kind, k],
                    turn_recv.at[kind, k], sp=z_flips[k] * PAIR + x,
                )
            )

    def pump(kind, k):
        here = region(kind, z_flips[k] * PAIR + x)
        if k:
            arrived(here, turn_recv.at[kind, k])
        send(
            remote(
                here if k else own_part(kind, z), here, pair_send.at[kind, k],
                pair_recv.at[kind, k], sp=mate,
            )
        )

    def paired(kind):
        for k in range(LINE):
            arrived(region(kind, z_flips[k] * PAIR + (PAIR - 1 - x)), pair_recv.at[kind, k])

    down_own = pl.ds(pl.multiple_of(x * down_hbm.shape[1], LANES), down_hbm.shape[1])
    down_mate = pl.ds(
        pl.multiple_of((PAIR - 1 - x) * down_hbm.shape[1], LANES), down_hbm.shape[1]
    )

    def pump_down(half):
        send(
            remote(
                down_hbm.at[down_part(half), :], down.at[down_part(half), down_own],
                down_send.at[half], down_recv.at[half], sp=mate,
            )
        )

    turn(0)
    turn(1)
    pump(0, 0)
    pump(1, 0)
    pump_down(0)
    own_copies = [local(own_part(kind, z), region(kind, rank), 3 + kind) for kind in range(2)]
    own_copies.append(local(down_hbm, down.at[:, down_own], 5))

    for head in range(heads):
        at = head * (NOPE + ROPE)
        rotary = turned(
            query_ref[:, at + NOPE : at + NOPE + ROPE].astype(jnp.float32), table_ref[:, :ROPE],
            table_ref[:, ROPE:],
        ).astype(jnp.bfloat16)
        query[head, :, :NOPE] = query_ref[:, at : at + NOPE]
        query[head, :, NOPE:] = jnp.concatenate([rotary, jnp.zeros_like(rotary)], axis=1)
    top[...] = jnp.full(top.shape, LOWEST, jnp.float32)
    norm[...] = jnp.zeros(norm.shape, jnp.float32)
    acc[...] = jnp.zeros(acc.shape, jnp.float32)
    scale = math.log2(math.e) / math.sqrt(NOPE + ROPE)
    kv_copy.wait()

    def attend(index, carry):
        source = rank - index

        @pl.when(index < rank)
        def _():
            arrived(lat_piece(source - 1, col), lat_recv.at[source - 1])
            piece = lat_piece(source - 1, col)
            lat_spread(source - 1, piece, 2, 2).start()
            lat_spread(source - 1, piece, 1, 1).start()

        arrived(lat_piece(source, col_flips[2]), lat_spread_recv.at[source, 1])
        lat_spread(source, lat_piece(source, col_flips[2]), 1, 3).start()
        arrived(lat_piece(source, col_flips[1]), lat_spread_recv.at[source, 0])
        arrived(lat_piece(source, col_flips[3]), lat_spread_recv.at[source, 2])
        key_value = jnp.dot(
            lat_buf[source, :, :latent], kv_w[...], preferred_element_type=jnp.float32
        ).astype(jnp.bfloat16)
        key_rope = lat_buf[source, :, latent:]
        row_of = lax.broadcasted_iota(jnp.int32, (rows, rows), 0) + index * rows
        allowed = lax.broadcasted_iota(jnp.int32, (rows, rows), 1) <= row_of
        for head in range(heads):
            at = head * (NOPE + VDIM)
            keys = jnp.concatenate([key_value[:, at : at + NOPE], key_rope], axis=1)
            scores = lax.dot_general(
                query[head], keys, (((1,), (1,)), ((), ())), preferred_element_type=jnp.float32
            )
            scores = jnp.where(allowed, scores * scale, LOWEST)
            old = top[head]
            new = jnp.maximum(old, jnp.max(scores, axis=1, keepdims=True))
            weights = jnp.exp2(scores - new[:, :1])
            fade = jnp.exp2(old - new)
            top[head] = new
            norm[head] = norm[head] * fade + jnp.sum(weights, axis=1, keepdims=True)
            across = slice(head * VDIM, (head + 1) * VDIM)
            acc[:, across] = acc[:, across] * fade + jnp.dot(
                weights.astype(jnp.bfloat16), key_value[:, at + NOPE : at + NOPE + VDIM],
                preferred_element_type=jnp.float32,
            )
        return carry

    lax.fori_loop(0, rank + 1, attend, 0)

    squares = jnp.zeros((rows, 1), jnp.float32)
    attended = []
    for head in range(heads):
        across = slice(head * VDIM, (head + 1) * VDIM)
        part = (acc[:, across] / norm[head]).astype(jnp.bfloat16).astype(jnp.float32)
        squares = squares + jnp.sum(part * part, axis=1, keepdims=True)
        attended.append((part * out_gain_ref[:, across]).astype(jnp.bfloat16))
    attended = jnp.concatenate(attended, axis=1)
    stats_mine[...] = jnp.broadcast_to(squares, stats_mine.shape)

    chunk = 4 * LANES

    def piece_of(ref, column):
        return ref.at[pl.ds(pl.multiple_of(column * share, share), share), :]

    def project(left, right, target):
        def one(index, carry):
            at = pl.ds(pl.multiple_of(index * chunk, chunk), chunk)
            target[:, at] = jnp.dot(
                left, right[:, at], preferred_element_type=jnp.float32
            ).astype(jnp.bfloat16)
            return carry

        lax.fori_loop(0, right.shape[1] // chunk, one, 0)

    def each_chunk(across, work):
        def one(index, carry):
            work(pl.ds(pl.multiple_of(index * chunk, chunk), chunk))
            return carry

        lax.fori_loop(0, across // chunk, one, 0)

    def fold(part, core, out, near, sems):
        core_s, core_r, near_s, near_r = sems
        for slot, column in ((1, 3), (0, 1)):
            send(
                remote(
                    piece_of(part, col_flips[column]), core.at[slot], core_s.at[slot],
                    core_r.at[slot], tp=col_flips[1],
                )
            )
        arrived(core.at[1], core_r.at[1])
        theirs = pl.ds(pl.multiple_of(col_flips[2] * share, share), share)

        def add(at):
            out[:, at] = (
                part[theirs, at].astype(jnp.float32) + core[1, :, at].astype(jnp.float32)
            ).astype(jnp.bfloat16)

        each_chunk(out.shape[1], add)
        send(remote(out, near, near_s, near_r, tp=col_flips[2]))
        arrived(core.at[0], core_r.at[0])

    def folded(part, core, near, sems, keep):
        arrived(near, sems[3])

        def add(at):
            keep(
                at,
                part[own_rows, at].astype(jnp.float32)
                + core[0, :, at].astype(jnp.float32)
                + near[:, at].astype(jnp.float32),
            )

        each_chunk(near.shape[1], add)

    out_copy.wait()
    for m in range(1, COLUMNS):
        send(
            remote(
                stats_mine.at[pl.ds(pl.multiple_of(col_flips[m] * share, share), share), :],
                stats_in.at[m - 1], stat_send.at[m - 1], stat_recv.at[m - 1], tp=col_flips[m],
            )
        )
    project(attended, out_w, partial)
    first = (core_send, core_recv, near_send.at[0], near_recv.at[0])
    fold(partial, core_in, near_out, near_in, first)
    pump(0, 1)
    squares = stats_mine[own_rows, :]
    for m in range(1, COLUMNS):
        arrived(stats_in.at[m - 1], stat_recv.at[m - 1])
        squares = squares + stats_in[m - 1]
    factor = lax.rsqrt(squares / (HEADS * VDIM) + EPSILON)[:, :1]

    def keep_total(at, values):
        total[:, at] = values

    folded(partial, core_in, near_in, first, keep_total)
    resid_copy.wait()
    squares = jnp.zeros((share, 1), jnp.float32)
    for index in range(width // chunk):
        at = slice(index * chunk, (index + 1) * chunk)
        mid = (resid[:, at].astype(jnp.float32) + total[:, at] * factor).astype(jnp.bfloat16)
        middle[:, at] = mid
        mid = mid.astype(jnp.float32)
        squares = squares + jnp.sum(mid * mid, axis=1, keepdims=True)
    factor = lax.rsqrt(squares / width + EPSILON)

    slab = width // PARTS

    def act_piece(place, column, part):
        at = pl.multiple_of(place * rows + column * share, share)
        return act.at[pl.ds(at, share), pl.ds(part * slab, slab)]

    at_own = pl.ds(pl.multiple_of(z * rows + col * share, share), share)
    for index in range(width // chunk):
        at = slice(index * chunk, (index + 1) * chunk)
        act[at_own, at] = (
            middle[:, at].astype(jnp.float32) * factor * ffn_gain_ref[:, at]
        ).astype(jnp.bfloat16)

    def up_line(src, dst, send_sem, recv_sem, when):
        send(remote(src, dst, send_sem, recv_sem, sp=(rank + PAIR) % ranks), when)

    def down_line(src, dst, send_sem, recv_sem, when):
        send(remote(src, dst, send_sem, recv_sem, sp=(rank + ranks - PAIR) % ranks), when)

    def act_spread(place, flip, slot, part):
        piece = act_piece(place, col_flips[slot - flip], part)
        send(
            remote(
                piece, piece, act_spread_send.at[place, slot - 1, part],
                act_spread_recv.at[place, slot - 1, part], tp=col_flips[flip],
            )
        )

    def act_line(place, index, part, up, lower):
        piece = act_piece(place, col, part)
        recv = act_line_recv.at[place, part]
        up_line(piece, piece, act_line_send.at[2 * index, part], recv, up)
        down_line(piece, piece, act_line_send.at[2 * index + 1, part], recv, lower)
        act_spread(place, 2, 2, part)
        act_spread(place, 1, 1, part)

    for part in range(PARTS):
        act_line(z, 0, part, z < LINE - 1, z > 0)
    pump(0, 2)
    pump(0, 3)

    def arrival(at):
        inside = ((at + 1) // 2) % 2
        half, mirror = (at + 2) % LINE, LINE - 1 - at
        return [
            at,
            at + 1 - 2 * (at % 2),
            half * (1 - inside) + mirror * inside,
            mirror * (1 - inside) + half * inside,
        ]

    order = arrival(z)

    def near_act(place, part):
        arrived(act_piece(place, col_flips[2], part), act_spread_recv.at[place, 1, part])
        act_spread(place, 1, 3, part)

    def next_act(index):
        nearer = order[index]
        for part in range(PARTS):
            arrived(act_piece(nearer, col, part), act_line_recv.at[nearer, part])
            act_line(
                nearer, index, part, (nearer < z) & (z < LINE - 1), (nearer > z) & (z > 0)
            )
            near_act(order[index - 1], part)

    next_act(1)
    for k in range(1, LINE):
        pump(1, k)
    pump_down(1)
    next_act(2)

    def hid_piece(place, source):
        return hidden.at[
            pl.ds(pl.multiple_of(place * rows, rows), rows),
            pl.ds(pl.multiple_of(source * units, units), units),
        ]

    def gated(index):
        place = order[index]
        for part in range(PARTS):
            arrived(act_piece(place, col_flips[1], part), act_spread_recv.at[place, 0, part])
            arrived(act_piece(place, col_flips[3], part), act_spread_recv.at[place, 2, part])
        here = pl.ds(pl.multiple_of(place * rows, rows), rows)
        both = jnp.dot(act[here, :], gate_up[...], preferred_element_type=jnp.float32)
        gate = both[:, :units]
        hidden[here, pl.ds(pl.multiple_of(z * units, units), units)] = (
            gate / (1.0 + jnp.exp(-gate)) * both[:, units:]
        ).astype(jnp.bfloat16)

    def leave(index):
        place = order[index]
        piece = hid_piece(place, z)
        up_line(piece, piece, hid_send.at[index, 0], hid_recv.at[place, z], z < LINE - 1)
        down_line(piece, piece, hid_send.at[index, 1], hid_recv.at[place, z], z > 0)

    def pass_hidden(index, distance):
        for side, source, when in (
            (0, z - distance, (z - distance >= 0) & (z < LINE - 1)),
            (1, z + distance, (z + distance < LINE) & (z > 0)),
        ):
            source = (source + LINE) % LINE
            place = arrival(source)[index]
            piece = hid_piece(place, source)
            copy = remote(
                piece, piece, hid_pass_send.at[index, distance - 1, side],
                hid_recv.at[place, source],
                sp=((rank + PAIR) if side == 0 else (rank + ranks - PAIR)) % ranks,
            )

            @pl.when(when)
            def _():
                arrived(piece, hid_recv.at[place, source])
                copy.start()

            pending.append((copy, when))

    upper = z // (LINE // 2)

    def row_place(index):
        return index * upper + (LINE - 1 - index) * (1 - upper)

    def hidden_all(index):
        place = row_place(index)
        for distance in range(1, LINE):
            for source, when in (
                (LINE - 1 - distance, z == LINE - 1),
                (distance, z == 0),
            ):

                @pl.when(when)
                def _():
                    arrived(hid_piece(place, source), hid_recv.at[place, source])

    def row_sems(index):
        return (
            core_rows_send.at[index], core_rows_recv.at[index], near_rows_send.at[index],
            near_rows_recv.at[index],
        )

    def start_rows(index):
        place = row_place(index)
        hidden_all(index)
        here = pl.ds(pl.multiple_of(place * rows, rows), rows)
        project(hidden[here, :], down, partial_rows.at[index])
        fold(
            partial_rows.at[index], core_rows.at[index], near_rows_out.at[index],
            near_rows_in.at[index], row_sems(index),
        )

    def end_rows(index):
        place = row_place(index)

        def keep(at, values):
            rows_out[index, :, at] = values.astype(jnp.bfloat16)

        folded(
            partial_rows.at[index], core_rows.at[index], near_rows_in.at[index], row_sems(index),
            keep,
        )
        send(
            remote(
                rows_out.at[index], rows_in.at[z], rows_send.at[index], rows_recv.at[z],
                sp=place * PAIR + x,
            ),
            z != place,
        )

        @pl.when(z == place)
        def _():
            rows_in[z] = rows_out[index]


    def weights_ready():
        for copy in own_copies:
            copy.wait()
        paired(0)
        paired(1)

    outer = (z == 0) | (z == LINE - 1)

    def early(first):
        weights_ready()
        for index in range(2):
            gated(index)
            place = order[index]
            piece = hid_piece(place, z)
            recv = hid_recv.at[place, z]
            up = remote(
                piece, piece, hid_send.at[index, 0], recv, sp=(rank + PAIR) % ranks
            )
            lower = remote(
                piece, piece, hid_send.at[index, 1], recv, sp=(rank + ranks - PAIR) % ranks
            )
            if first:
                pl.when(z == 0)(up.start)
                pl.when(z > 0)(lower.start)
            else:
                up.start()
                lower.start()

    pl.when(outer)(functools.partial(early, True))
    next_act(3)
    pl.when(inner > 0)(functools.partial(early, False))
    for index in range(2):
        piece = hid_piece(order[index], z)
        for side, when in ((0, z < LINE - 1), (1, z > 0)):
            pending.append(
                (remote(piece, piece, hid_send.at[index, side], hid_send.at[index, side],
                        sp=mate), when)
            )
    gated(2)
    leave(2)
    for part in range(PARTS):
        near_act(order[LINE - 1], part)
    gated(3)
    leave(3)
    pass_hidden(0, 1)
    pass_hidden(1, 1)
    pass_hidden(0, 2)
    pass_hidden(2, 1)
    pass_hidden(1, 2)
    pass_hidden(3, 1)
    pass_hidden(2, 2)
    pass_hidden(3, 2)
    for half in range(2):
        arrived(down.at[down_part(half), down_mate], down_recv.at[half])
    start_rows(0)
    start_rows(1)
    end_rows(0)
    start_rows(2)
    end_rows(1)
    start_rows(3)
    end_rows(2)
    end_rows(3)
    for source in range(LINE):

        @pl.when(z != source)
        def _():
            arrived(rows_in.at[source], rows_recv.at[source])

    part = rows_in.shape[2]
    for source in range(LINE):
        at = slice(source * part, (source + 1) * part)
        result_ref[:, at] = (
            middle[:, at].astype(jnp.float32) + rows_in[source].astype(jnp.float32)
        ).astype(jnp.bfloat16)

    for copy, when in pending:
        if when is None:
            copy.wait_send()
        else:
            pl.when(when)(copy.wait_send)

    def drain(source, carry):
        piece = lat_piece(source, col)
        for slot in range(COLUMNS - 1):
            remote(
                piece, piece, lat_spread_send.at[source, slot], lat_spread_send.at[source, slot],
                tp=col_flips[1],
            ).wait_send()
        return carry

    lax.fori_loop(0, rank + 1, drain, 0)


def fused_body(
    resid,
    queries,
    latent,
    rope_key,
    lat_gain,
    kv_weight,
    out_gain,
    out_weight,
    ffn_gain,
    gate_weight,
    up_weight,
    down_weight,
):
    ranks, columns = lax.axis_size("sp"), lax.axis_size("tp")
    rank = lax.axis_index("sp")
    rows, width = resid.shape
    share = rows // columns
    heads = queries.shape[1] // (NOPE + ROPE)
    units = gate_weight.shape[1] // LINE
    block = gate_weight.shape[0]
    depth = latent.shape[1]
    places = (rank * rows + jnp.arange(rows, dtype=jnp.int32)).astype(jnp.float32)
    half = ROPE // 2
    inverse = THETA ** (-jnp.arange(half, dtype=jnp.float32) / half)
    angle = places[:, None] * inverse
    cosine, sine = jnp.cos(angle), jnp.sin(angle)
    table = jnp.concatenate([cosine, cosine, -sine, sine], axis=1)
    bf, f32 = jnp.bfloat16, jnp.float32
    dma = pltpu.SemaphoreType.DMA
    vmem = pl.BlockSpec(memory_space=pltpu.VMEM)
    anywhere = pl.BlockSpec(memory_space=pl.ANY)
    part = width // LINE
    others = columns - 1
    return pl.pallas_call(
        whole_step,
        out_shape=jax.ShapeDtypeStruct((share, width), bf),
        in_specs=[vmem] * 7 + [anywhere] * 6,
        out_specs=vmem,
        scratch_shapes=[
            pltpu.VMEM((share, depth + LANES), bf),
            pltpu.VMEM((ranks, rows, depth + LANES), bf),
            pltpu.VMEM((heads, rows, 2 * LANES), bf),
            pltpu.VMEM((share, width), bf),
            pltpu.VMEM(kv_weight.shape, bf),
            pltpu.VMEM(out_weight.shape, bf),
            pltpu.VMEM((ranks * block, 2 * units), bf),
            pltpu.VMEM((LINE * units, PAIR * down_weight.shape[1]), bf),
            pltpu.VMEM((LINE * rows, width), bf),
            pltpu.VMEM((LINE * rows, LINE * units), bf),
            pltpu.VMEM((heads, rows, LANES), f32),
            pltpu.VMEM((heads, rows, LANES), f32),
            pltpu.VMEM((rows, heads * VDIM), f32),
            pltpu.VMEM((rows, LANES), f32),
            pltpu.VMEM((others, share, LANES), f32),
            pltpu.VMEM((rows, width), bf),
            pltpu.VMEM((2, share, width), bf),
            pltpu.VMEM((share, width), bf),
            pltpu.VMEM((share, width), bf),
            pltpu.VMEM((LINE, rows, part), bf),
            pltpu.VMEM((LINE, 2, share, part), bf),
            pltpu.VMEM((LINE, share, part), bf),
            pltpu.VMEM((LINE, share, part), bf),
            pltpu.VMEM((LINE, share, part), bf),
            pltpu.VMEM((LINE, share, part), bf),
            pltpu.VMEM((share, width), bf),
            pltpu.VMEM((share, width), f32),
            dma((6,)),
            dma((ranks - 1,)),
            dma((ranks,)),
            dma((ranks, others)),
            dma((ranks, others)),
            dma((2, LINE)),
            dma((2, LINE)),
            dma((2, LINE)),
            dma((2, LINE)),
            dma((2,)),
            dma((2,)),
            dma((2 * LINE, PARTS)),
            dma((LINE, PARTS)),
            dma((LINE, others, PARTS)),
            dma((LINE, others, PARTS)),
            dma((others,)),
            dma((others,)),
            dma((2,)),
            dma((2,)),
            dma((1,)),
            dma((1,)),
            dma((LINE, 2)),
            dma((LINE, 2, 2)),
            dma((LINE, LINE)),
            dma((LINE, 2)),
            dma((LINE, 2)),
            dma((LINE,)),
            dma((LINE,)),
            dma((LINE,)),
            dma((LINE,)),
        ],
        compiler_params=pltpu.CompilerParams(
            collective_id=0, has_side_effects=True, vmem_limit_bytes=66 * 1024 * 1000
        ),
    )(
        queries,
        latent,
        rope_key,
        table,
        lat_gain.reshape(1, -1),
        out_gain.reshape(1, -1),
        ffn_gain.reshape(1, -1),
        resid,
        kv_weight,
        out_weight,
        gate_weight,
        up_weight,
        down_weight,
    )


def solution(mesh):
    placed = (
        P("sp", None),
        P("sp", "tp"),
        P("sp", None),
        P("sp", None),
        P(),
        P(None, "tp"),
        P("tp"),
        P("tp", None),
        P(),
        P("sp", "tp"),
        P("sp", "tp"),
        P("tp", "sp"),
    )

    def mapped(function):
        return jax.shard_map(
            function, mesh=mesh, in_specs=placed, out_specs=P(("sp", "tp"), None), check_vma=False
        )

    if mesh.shape["sp"] == PAIR * LINE and mesh.shape["tp"] == COLUMNS:
        return mapped(fused_body)
    return mapped(plain_body)
```

```python
import functools
import math

import jax
import jax.numpy as jnp
from jax import lax
from jax.experimental import pallas as pl
from jax.experimental.pallas import tpu as pltpu
from jax.sharding import PartitionSpec as P


HEADS = 16
NOPE = 128
ROPE = 64
VDIM = 128


EPSILON = 1e-06
THETA = 10000.0
LOWEST = -1e30
GROUP = 4


def rotate(values, places):
    half = values.shape[-1] // 2
    inverse = THETA ** (-jnp.arange(half, dtype=jnp.float32) / half)
    angle = places[..., None] * inverse
    cosine = jnp.cos(angle)
    sine = jnp.sin(angle)
    first = values[..., :half]
    second = values[..., half:]
    return jnp.concatenate(
        [first * cosine - second * sine, first * sine + second * cosine], axis=-1
    )


def norm_rows(values, gain):
    wide = values.astype(jnp.float32)
    return wide * lax.rsqrt(jnp.mean(wide * wide, axis=-1, keepdims=True) + EPSILON) * gain


def make_keys(latent_piece, rotary_piece, lat_gain, kv_weight, key_index):
    normed = norm_rows(latent_piece, lat_gain).astype(jnp.bfloat16)
    key_value = jnp.dot(normed, kv_weight, preferred_element_type=jnp.float32)
    key_value = key_value.astype(jnp.bfloat16)
    key_rope = rotate(rotary_piece.astype(jnp.float32), key_index.astype(jnp.float32)).astype(
        jnp.bfloat16
    )
    return (key_value, key_rope)


def to_near(values, flip):
    ranks = lax.axis_size("sp")
    return lax.ppermute(values, "sp", [(rank, rank ^ flip) for rank in range(ranks)])


def to_high(values, step, ranks):
    if step % (ranks // GROUP) == 0:
        return values
    return lax.ppermute(
        values, "sp", [(rank, (rank + step * GROUP) % ranks) for rank in range(ranks)]
    )


def reorder(blocks, place):
    bit = 1
    while bit < len(blocks):
        swap = place // bit % 2 == 1
        blocks = [jnp.where(swap, blocks[j ^ bit], blocks[j]) for j in range(len(blocks))]
        bit *= 2
    return blocks


def by_distance(values, place):
    return jnp.concatenate(reorder(jnp.split(values, GROUP, axis=1), place), axis=1)


def to_column(values, bit):
    columns = lax.axis_size("tp")
    return lax.ppermute(values, "tp", [(column, column ^ bit) for column in range(columns)])


def gather_columns(values):
    rows = values.shape[0]
    held = {0: values}
    bit = lax.axis_size("tp") // 2
    while bit:
        keys = sorted(held)
        theirs = to_column(jnp.concatenate([held[key] for key in keys], axis=0), bit)
        for at, key in enumerate(keys):
            held[key + bit] = theirs[at * rows : (at + 1) * rows]
        bit //= 2
    return jnp.concatenate([held[key] for key in sorted(held)], axis=0)


def scatter_columns(values):
    columns = lax.axis_size("tp")
    blocks = dict(enumerate(jnp.split(values, columns, axis=0)))
    bit = 1
    while bit < columns:
        mine = [key for key in sorted(blocks) if not key & bit]
        theirs = to_column(jnp.concatenate([blocks[key + bit] for key in mine], axis=0), bit)
        theirs = jnp.split(theirs, len(mine), axis=0)
        blocks = {
            key: (blocks[key].astype(jnp.float32) + piece.astype(jnp.float32)).astype(jnp.bfloat16)
            for key, piece in zip(mine, theirs)
        }
        bit *= 2
    return blocks[0]


def near_weights(gate, up, down):
    gate_one = to_near(gate, 1)
    up_two = to_near(up, 2)
    up_one = to_near(up, 1)
    gate_two = to_near(gate, 2)
    gate_both = to_near(gate_one, 2)
    up_both = to_near(up_two, 1)
    down, gate_both, up_both = lax.optimization_barrier((down, gate_both, up_both))
    half = down.shape[0] // 2
    down_one = to_near(down, 1)
    down_two = to_near(down, 2)
    far = [to_near(down_one[:half], 2), to_near(down_two[half:], 1)]
    down_both = jnp.concatenate(far, axis=0)
    return (
        (gate, gate_one, gate_two, gate_both),
        (up, up_one, up_two, up_both),
        (down, down_one, down_two, down_both),
    )


def blocks_dot(rows, weights, block):
    return sum(
        jnp.dot(
            rows[:, place * block : (place + 1) * block], weight, preferred_element_type=jnp.float32
        )
        for place, weight in enumerate(weights)
    )


def plain_body(
    resid,
    queries,
    latent,
    rope_key,
    lat_gain,
    kv_weight,
    out_gain,
    out_weight,
    ffn_gain,
    gate_weight,
    up_weight,
    down_weight,
):
    gate_blocks, up_blocks, down_blocks = near_weights(gate_weight, up_weight, down_weight)
    rows_here = resid.shape[0]
    first_row = lax.axis_index("sp") * rows_here
    heads_here = queries.shape[1] // (NOPE + ROPE)
    columns = lax.axis_size("tp")
    column = lax.axis_index("tp")
    share = rows_here // columns
    query = jnp.concatenate(reorder(jnp.split(queries, columns, axis=0), column), axis=0)
    query = query.reshape(rows_here, heads_here, NOPE + ROPE)
    within = jnp.arange(rows_here, dtype=jnp.int32)
    own_columns = (within // share) ^ column
    query_index = first_row + own_columns * share + within % share
    query_nope = query[:, :, :NOPE]
    query_rope = rotate(
        query[:, :, NOPE:].astype(jnp.float32), query_index.astype(jnp.float32)[:, None]
    ).astype(jnp.bfloat16)
    scale = 1.0 / math.sqrt(NOPE + ROPE)

    def accumulate(state, key_value, key_rope):
        running_max, running_sum, weighted = state
        length = key_value.shape[0]
        key_value = key_value.reshape(length, heads_here, NOPE + VDIM)
        scores = jnp.einsum(
            "qhd,khd->hqk", query_nope, key_value[:, :, :NOPE], preferred_element_type=jnp.float32
        )
        scores = (
            scores
            + jnp.einsum("qhr,kr->hqk", query_rope, key_rope, preferred_element_type=jnp.float32)
        ) * scale
        allowed = (key_index[None, :] <= query_index[:, None])[None]
        scores = jnp.where(allowed, scores, LOWEST)
        new_max = jnp.maximum(running_max, jnp.max(scores, axis=-1))
        weights = jnp.where(allowed, jnp.exp(scores - new_max[:, :, None]), 0.0)
        running_sum = jnp.sum(weights, axis=-1)
        added = jnp.einsum(
            "hqk,khd->qhd",
            weights.astype(jnp.bfloat16),
            key_value[:, :, NOPE:],
            preferred_element_type=jnp.float32,
        )
        weighted = added
        return (new_max, running_sum, weighted)

    initial = (
        jnp.full((heads_here, rows_here), LOWEST, jnp.float32),
        jnp.zeros((heads_here, rows_here), jnp.float32),
        jnp.zeros((rows_here, heads_here, VDIM), jnp.float32),
    )
    ranks = lax.axis_size("sp")
    rank = lax.axis_index("sp")
    both = jnp.concatenate([latent, rope_key], axis=1)
    both = lax.dynamic_slice_in_dim(both, column * share, share, 0)
    pieces = [both]
    for step in range(1, ranks):
        onward = [(source, source + step) for source in range(ranks - step)]
        pieces.append(lax.ppermute(both, "sp", onward))
    both = gather_columns(jnp.concatenate(pieces, axis=0))
    within = jnp.arange(both.shape[0], dtype=jnp.int32)
    source = (rank - within // share % ranks + ranks) % ranks
    key_index = source * rows_here + ((within // (share * ranks)) ^ column) * share + within % share
    pieces = (both[:, : latent.shape[1]], both[:, latent.shape[1] :])

    def update(state):
        key_value, key_rope = make_keys(pieces[0], pieces[1], lat_gain, kv_weight, key_index)
        return accumulate(state, key_value, key_rope)

    _, running_sum, weighted = update(initial)
    attended = (weighted / jnp.transpose(running_sum)[:, :, None]).astype(jnp.bfloat16)
    attended_float = attended.reshape(rows_here, heads_here * VDIM).astype(jnp.float32)
    squares = jnp.split(jnp.sum(attended_float * attended_float, axis=1), columns)
    squares = lax.psum(jnp.concatenate(reorder(squares, column)), "tp")
    squares = jnp.concatenate(reorder(jnp.split(squares, columns), column))
    normed_out = attended_float * lax.rsqrt(squares / (HEADS * VDIM) + EPSILON)[:, None] * out_gain
    normed_out = normed_out.astype(jnp.bfloat16)
    own_first = lax.axis_index("tp") * share
    projected = jnp.dot(normed_out, out_weight, preferred_element_type=jnp.float32)
    projected = projected.astype(jnp.bfloat16)
    attn_sum = scatter_columns(projected).astype(jnp.float32)
    own_resid = lax.dynamic_slice_in_dim(resid, own_first, share, 0)
    middle = (own_resid.astype(jnp.float32) + attn_sum).astype(jnp.bfloat16)
    highs = ranks // GROUP
    high = rank // GROUP
    place = rank % GROUP
    width = resid.shape[1]
    block = width // ranks
    wide = GROUP * block
    mids = norm_rows(middle, ffn_gain).astype(jnp.bfloat16)
    mids = [
        to_high(
            by_distance(
                lax.dynamic_slice_in_dim(mids, (high + step) % highs * wide, wide, 1), place
            ),
            step,
            ranks,
        )
        for step in range(highs)
    ]
    mids = [gather_columns(piece) for piece in mids]
    gates, ups = None, None
    for step in list(range(1, highs)) + [0]:
        piece = mids[step]
        gate = blocks_dot(piece, gate_blocks, block)
        up = blocks_dot(piece, up_blocks, block)
        if step:
            gate = to_high(gate.astype(jnp.bfloat16), highs - step, ranks).astype(jnp.float32)
            up = to_high(up.astype(jnp.bfloat16), highs - step, ranks).astype(jnp.float32)
        gates = gate if gates is None else gates + gate
        ups = up if ups is None else ups + up
    hidden = (jax.nn.silu(gates) * ups).astype(jnp.bfloat16)
    received = [to_high(hidden, step, ranks) for step in range(highs)]
    terms = []
    for step in range(highs):
        partial = jnp.concatenate(
            [
                jnp.dot(received[step], weight, preferred_element_type=jnp.float32).astype(
                    jnp.bfloat16
                )
                for weight in down_blocks
            ],
            axis=1,
        )
        partial = to_high(scatter_columns(partial), highs - step, ranks)
        terms.append(by_distance(partial, place))
    terms = jnp.concatenate(terms, axis=1)
    ffn_sum = jnp.concatenate(
        [
            lax.dynamic_slice_in_dim(terms, (index - high + highs) % highs * wide, wide, 1)
            for index in range(highs)
        ],
        axis=1,
    ).astype(jnp.float32)
    return (middle.astype(jnp.float32) + ffn_sum).astype(jnp.bfloat16)


LANES = 128
PAIR = 2
LINE = 4
COLUMNS = 4
MESH = pl.DeviceIdType.MESH


PARTS = 4


def whole_step(
    query_ref,
    latent_ref,
    inverse_ref,
    lat_gain_ref,
    out_gain_ref,
    ffn_gain_ref,
    rope_hbm,
    resid_hbm,
    kv_hbm,
    out_hbm,
    gate_hbm,
    up_hbm,
    down_hbm,
    result_ref,
    lat_mine,
    rope_mine,
    lat_buf,
    query,
    resid,
    kv_w,
    out_w,
    gate_up,
    down,
    act,
    hidden,
    top,
    norm,
    acc,
    stats_mine,
    stats_in,
    partial,
    core_in,
    near_out,
    near_in,
    partial_rows,
    core_rows,
    near_rows_out,
    near_rows_in,
    rows_out,
    rows_in,
    middle,
    total,
    local_sem,
    lat_send,
    lat_recv,
    lat_pass_send,
    lat_spread_send,
    lat_spread_recv,
    turn_send,
    turn_recv,
    pair_send,
    pair_recv,
    down_send,
    down_recv,
    act_line_send,
    act_line_recv,
    act_spread_send,
    act_spread_recv,
    stat_send,
    stat_recv,
    core_send,
    core_recv,
    near_send,
    near_recv,
    hid_send,
    hid_pass_send,
    hid_recv,
    core_rows_send,
    core_rows_recv,
    near_rows_send,
    near_rows_recv,
    rows_send,
    rows_recv,
):
    rank = lax.axis_index("sp")
    col = lax.axis_index("tp")
    ranks = lat_buf.shape[0]
    rows = lat_buf.shape[1]
    share = lat_mine.shape[0]
    width = resid.shape[1]
    units = hidden.shape[1] // LINE
    block = gate_hbm.shape[0]
    latent = kv_w.shape[0]
    heads = query.shape[0]
    z = rank // PAIR
    x = rank % PAIR
    mate = z * PAIR + (PAIR - 1 - x)
    inner = ((z + 1) // 2) % 2
    z_flips = [z, z + 1 - 2 * (z % 2), (z + 2) % LINE, LINE - 1 - z]
    col_flips = [col, col + 1 - 2 * (col % 2), (col + 2) % COLUMNS, COLUMNS - 1 - col]
    pending = []

    def remote(src, dst, send, recv, sp=None, tp=None):
        target = (rank if sp is None else sp, col if tp is None else tp)
        return pltpu.make_async_remote_copy(
            src_ref=src, dst_ref=dst, send_sem=send, recv_sem=recv, device_id=target,
            device_id_type=MESH,
        )

    def arrived(dst, recv):
        remote(dst, dst, recv, recv, tp=col_flips[1]).wait_recv()

    def send(copy, when=None):
        if when is None:
            copy.start()
        else:
            pl.when(when)(copy.start)
        pending.append((copy, when))

    def local(src, dst, slot):
        copy = pltpu.make_async_copy(src, dst, local_sem.at[slot])
        copy.start()
        return copy

    own_rows = pl.ds(pl.multiple_of(col * share, share), share)
    rope_copy = local(rope_hbm.at[own_rows, :], rope_mine, 8)
    barrier = pltpu.get_barrier_semaphore()
    for step in range(1, ranks):
        pl.semaphore_signal(
            barrier, inc=1, device_id=((rank + step) % ranks, col), device_id_type=MESH
        )
    for flip in col_flips[1:]:
        pl.semaphore_signal(barrier, inc=1, device_id=(rank, flip), device_id_type=MESH)
    kv_copy = local(kv_hbm, kv_w, 0)
    out_copy = local(out_hbm, out_w, 1)
    resid_copy = local(resid_hbm.at[own_rows, :], resid, 2)

    def turned(values, cosine, sine):
        half = values.shape[1] // 2
        swapped = jnp.concatenate([values[:, half:], values[:, :half]], axis=1)
        return values * cosine + swapped * sine

    def table(start, count):
        shape = (count, ROPE)
        place = (start + lax.broadcasted_iota(jnp.int32, shape, 0)).astype(jnp.float32)
        angle = place * inverse_ref[...]
        sine = jnp.sin(angle)
        low = lax.broadcasted_iota(jnp.int32, shape, 1) < ROPE // 2
        return jnp.cos(angle), jnp.where(low, -sine, sine)

    wide = latent_ref[own_rows, :].astype(jnp.float32)
    wide = wide * lax.rsqrt(jnp.mean(wide * wide, axis=1, keepdims=True) + EPSILON)
    lat_mine[:, :latent] = (wide * lat_gain_ref[...]).astype(jnp.bfloat16)
    cosine, sine = table(rank * rows + col * share, share)
    rope_copy.wait()
    key_rope = turned(rope_mine[...].astype(jnp.float32), cosine, sine).astype(jnp.bfloat16)
    lat_mine[:, latent:] = jnp.concatenate([key_rope, jnp.zeros_like(key_rope)], axis=1)

    pl.semaphore_wait(barrier, ranks - 1 + COLUMNS - 1)

    def lat_piece(source, column):
        return lat_buf.at[source, pl.ds(pl.multiple_of(column * share, share), share), :]

    def lat_spread(source, piece, flip, slot):
        return remote(
            piece, lat_piece(source, col_flips[slot - flip]),
            lat_spread_send.at[source, slot - 1], lat_spread_recv.at[source, slot - 1],
            tp=col_flips[flip],
        )

    for step in range(1, LINE):
        send(
            remote(
                lat_mine, lat_piece(rank, col), lat_send.at[step - 1], lat_recv.at[rank],
                sp=(rank + PAIR * step) % ranks,
            ),
            z + step < LINE,
        )
    send(
        remote(
            lat_mine, lat_piece(rank, col), lat_send.at[LINE - 1], lat_recv.at[rank], sp=mate
        ),
        x == 0,
    )
    lat_spread(rank, lat_mine, 2, 2).start()
    lat_spread(rank, lat_mine, 1, 1).start()
    lat_buf[rank, own_rows, :] = lat_mine[...]

    def region(kind, source):
        at = pl.multiple_of(source * block, block)
        return gate_up.at[pl.ds(at, block), pl.ds(kind * units, units)]

    def own_part(kind, place):
        at = pl.multiple_of(place * units, units)
        return (gate_hbm, up_hbm)[kind].at[:, pl.ds(at, units)]

    def down_part(half):
        middle_row = down_hbm.shape[0] // 2
        return pl.ds(half * middle_row, middle_row)

    def turn(kind):
        for k in range(1, LINE):
            send(
                remote(
                    own_part(kind, z_flips[k]), region(kind, rank), turn_send.at[kind, k],
                    turn_recv.at[kind, k], sp=z_flips[k] * PAIR + x,
                )
            )

    def pump(kind, k):
        here = region(kind, z_flips[k] * PAIR + x)
        if k:
            arrived(here, turn_recv.at[kind, k])
        send(
            remote(
                here if k else own_part(kind, z), here, pair_send.at[kind, k],
                pair_recv.at[kind, k], sp=mate,
            )
        )

    def paired(kind):
        for k in range(LINE):
            arrived(region(kind, z_flips[k] * PAIR + (PAIR - 1 - x)), pair_recv.at[kind, k])

    down_own = pl.ds(pl.multiple_of(x * down_hbm.shape[1], LANES), down_hbm.shape[1])
    down_mate = pl.ds(
        pl.multiple_of((PAIR - 1 - x) * down_hbm.shape[1], LANES), down_hbm.shape[1]
    )

    def pump_down(half):
        send(
            remote(
                down_hbm.at[down_part(half), :], down.at[down_part(half), down_own],
                down_send.at[half], down_recv.at[half], sp=mate,
            )
        )

    turn(0)
    turn(1)
    own_pumps = []
    own_copies = [local(own_part(kind, z), region(kind, rank), 3 + kind) for kind in range(2)]
    own_copies.append(local(down_hbm, down.at[:, down_own], 5))

    cosine, sine = table(rank * rows, rows)
    for head in range(heads):
        at = head * (NOPE + ROPE)
        rotary = turned(
            query_ref[:, at + NOPE : at + NOPE + ROPE].astype(jnp.float32), cosine, sine
        ).astype(jnp.bfloat16)
        query[head, :, :NOPE] = query_ref[:, at : at + NOPE]
        query[head, :, NOPE:] = jnp.concatenate([rotary, jnp.zeros_like(rotary)], axis=1)
    top[...] = jnp.full(top.shape, LOWEST, jnp.float32)
    norm[...] = jnp.zeros(norm.shape, jnp.float32)
    acc[...] = jnp.zeros(acc.shape, jnp.float32)
    scale = math.log2(math.e) / math.sqrt(NOPE + ROPE)
    kv_copy.wait()

    def lat_taken(source):
        piece = lat_piece(source, col)
        arrived(piece, lat_recv.at[source])
        lat_spread(source, piece, 2, 2).start()
        lat_spread(source, piece, 1, 1).start()

    def lat_onward(place):
        piece = lat_piece(place * PAIR + x, col)
        return remote(
            piece, piece, lat_pass_send.at[place], lat_recv.at[place * PAIR + x], sp=mate
        )

    for kind in range(2):
        here = region(kind, rank)
        own_pumps.append(
            remote(
                own_part(kind, z), here, pair_send.at[kind, 0], pair_recv.at[kind, 0], sp=mate
            )
        )
    own_pumps.append(
        remote(
            down_hbm.at[down_part(0), :], down.at[down_part(0), down_own], down_send.at[0],
            down_recv.at[0], sp=mate,
        )
    )
    pending += [(copy, None) for copy in own_pumps]

    def attend(index, carry):
        source = rank - index

        @pl.when((index < rank) & ((source - 1) % PAIR != x) & (index + x > 0))
        def _():
            lat_taken(source - 1)

        arrived(lat_piece(source, col_flips[2]), lat_spread_recv.at[source, 1])
        lat_spread(source, lat_piece(source, col_flips[2]), 1, 3).start()
        arrived(lat_piece(source, col_flips[1]), lat_spread_recv.at[source, 0])
        arrived(lat_piece(source, col_flips[3]), lat_spread_recv.at[source, 2])
        key_value = jnp.dot(
            lat_buf[source, :, :latent], kv_w[...], preferred_element_type=jnp.float32
        ).astype(jnp.bfloat16)
        key_rope = lat_buf[source, :, latent:]
        row_of = lax.broadcasted_iota(jnp.int32, (rows, rows), 0) + index * rows
        allowed = lax.broadcasted_iota(jnp.int32, (rows, rows), 1) <= row_of
        for head in range(heads):
            at = head * (NOPE + VDIM)
            keys = jnp.concatenate([key_value[:, at : at + NOPE], key_rope], axis=1)
            scores = lax.dot_general(
                query[head], keys, (((1,), (1,)), ((), ())), preferred_element_type=jnp.float32
            )
            scores = jnp.where(allowed, scores * scale, LOWEST)
            old = top[head]
            new = jnp.maximum(old, jnp.max(scores, axis=1, keepdims=True))
            weights = jnp.exp2(scores - new[:, :1])
            fade = jnp.exp2(old - new)
            top[head] = new
            norm[head] = norm[head] * fade + jnp.sum(weights, axis=1, keepdims=True)
            across = slice(head * VDIM, (head + 1) * VDIM)
            acc[:, across] = acc[:, across] * fade + jnp.dot(
                weights.astype(jnp.bfloat16), key_value[:, at + NOPE : at + NOPE + VDIM],
                preferred_element_type=jnp.float32,
            )

        @pl.when(index == 0)
        def _():
            def onward(step, carry):
                lat_taken((z - 1 - step) * PAIR + x)
                lat_onward(z - 1 - step).start()
                return carry

            lax.fori_loop(0, z, onward, 0)

            @pl.when((x == 0) & (rank > 0))
            def _():
                lat_taken(rank - 1)

            for copy in own_pumps:
                copy.start()

        return carry

    lax.fori_loop(0, rank + 1, attend, 0)

    squares = jnp.zeros((rows, 1), jnp.float32)
    attended = []
    for head in range(heads):
        across = slice(head * VDIM, (head + 1) * VDIM)
        part = (acc[:, across] / norm[head]).astype(jnp.bfloat16).astype(jnp.float32)
        squares = squares + jnp.sum(part * part, axis=1, keepdims=True)
        attended.append((part * out_gain_ref[:, across]).astype(jnp.bfloat16))
    attended = jnp.concatenate(attended, axis=1)
    stats_mine[...] = jnp.broadcast_to(squares, stats_mine.shape)

    chunk = 4 * LANES

    def piece_of(ref, column):
        return ref.at[pl.ds(pl.multiple_of(column * share, share), share), :]

    def project(left, right, target):
        def one(index, carry):
            at = pl.ds(pl.multiple_of(index * chunk, chunk), chunk)
            target[:, at] = jnp.dot(
                left, right[:, at], preferred_element_type=jnp.float32
            ).astype(jnp.bfloat16)
            return carry

        lax.fori_loop(0, right.shape[1] // chunk, one, 0)

    def each_chunk(across, work):
        def one(index, carry):
            work(pl.ds(pl.multiple_of(index * chunk, chunk), chunk))
            return carry

        lax.fori_loop(0, across // chunk, one, 0)

    def fold(part, core, out, near, sems):
        core_s, core_r, near_s, near_r = sems
        for slot, column in ((1, 3), (0, 1)):
            send(
                remote(
                    piece_of(part, col_flips[column]), core.at[slot], core_s.at[slot],
                    core_r.at[slot], tp=col_flips[1],
                )
            )
        arrived(core.at[1], core_r.at[1])
        theirs = pl.ds(pl.multiple_of(col_flips[2] * share, share), share)

        def add(at):
            out[:, at] = (
                part[theirs, at].astype(jnp.float32) + core[1, :, at].astype(jnp.float32)
            ).astype(jnp.bfloat16)

        each_chunk(out.shape[1], add)
        send(remote(out, near, near_s, near_r, tp=col_flips[2]))
        arrived(core.at[0], core_r.at[0])

    def folded(part, core, near, sems, keep):
        arrived(near, sems[3])

        def add(at):
            keep(
                at,
                part[own_rows, at].astype(jnp.float32)
                + core[0, :, at].astype(jnp.float32)
                + near[:, at].astype(jnp.float32),
            )

        each_chunk(near.shape[1], add)

    out_copy.wait()
    for m in range(1, COLUMNS):
        send(
            remote(
                stats_mine.at[pl.ds(pl.multiple_of(col_flips[m] * share, share), share), :],
                stats_in.at[m - 1], stat_send.at[m - 1], stat_recv.at[m - 1], tp=col_flips[m],
            )
        )
    project(attended, out_w, partial)
    first = (core_send, core_recv, near_send.at[0], near_recv.at[0])
    fold(partial, core_in, near_out, near_in, first)
    pump(0, 1)
    squares = stats_mine[own_rows, :]
    for m in range(1, COLUMNS):
        arrived(stats_in.at[m - 1], stat_recv.at[m - 1])
        squares = squares + stats_in[m - 1]
    factor = lax.rsqrt(squares / (HEADS * VDIM) + EPSILON)[:, :1]

    def keep_total(at, values):
        total[:, at] = values

    folded(partial, core_in, near_in, first, keep_total)
    resid_copy.wait()
    squares = jnp.zeros((share, 1), jnp.float32)
    for index in range(width // chunk):
        at = slice(index * chunk, (index + 1) * chunk)
        mid = (resid[:, at].astype(jnp.float32) + total[:, at] * factor).astype(jnp.bfloat16)
        middle[:, at] = mid
        mid = mid.astype(jnp.float32)
        squares = squares + jnp.sum(mid * mid, axis=1, keepdims=True)
    factor = lax.rsqrt(squares / width + EPSILON)

    slab = width // PARTS

    def act_piece(place, column, part):
        at = pl.multiple_of(place * rows + column * share, share)
        return act.at[pl.ds(at, share), pl.ds(part * slab, slab)]

    at_own = pl.ds(pl.multiple_of(z * rows + col * share, share), share)
    for index in range(width // chunk):
        at = slice(index * chunk, (index + 1) * chunk)
        act[at_own, at] = (
            middle[:, at].astype(jnp.float32) * factor * ffn_gain_ref[:, at]
        ).astype(jnp.bfloat16)

    def up_line(src, dst, send_sem, recv_sem, when):
        send(remote(src, dst, send_sem, recv_sem, sp=(rank + PAIR) % ranks), when)

    def down_line(src, dst, send_sem, recv_sem, when):
        send(remote(src, dst, send_sem, recv_sem, sp=(rank + ranks - PAIR) % ranks), when)

    def act_spread(place, flip, slot, part):
        piece = act_piece(place, col_flips[slot - flip], part)
        send(
            remote(
                piece, piece, act_spread_send.at[place, slot - 1, part],
                act_spread_recv.at[place, slot - 1, part], tp=col_flips[flip],
            )
        )

    def act_line(place, index, part, up, lower):
        piece = act_piece(place, col, part)
        recv = act_line_recv.at[place, part]
        up_line(piece, piece, act_line_send.at[2 * index, part], recv, up)
        down_line(piece, piece, act_line_send.at[2 * index + 1, part], recv, lower)
        act_spread(place, 2, 2, part)
        act_spread(place, 1, 1, part)

    for part in range(PARTS):
        act_line(z, 0, part, z < LINE - 1, z > 0)
    pump(0, 2)
    pump(0, 3)

    def arrival(at):
        inside = ((at + 1) // 2) % 2
        half, mirror = (at + 2) % LINE, LINE - 1 - at
        return [
            at,
            at + 1 - 2 * (at % 2),
            half * (1 - inside) + mirror * inside,
            mirror * (1 - inside) + half * inside,
        ]

    order = arrival(z)

    def near_act(place, part):
        arrived(act_piece(place, col_flips[2], part), act_spread_recv.at[place, 1, part])
        act_spread(place, 1, 3, part)

    def next_act(index):
        nearer = order[index]
        for part in range(PARTS):
            arrived(act_piece(nearer, col, part), act_line_recv.at[nearer, part])
            act_line(
                nearer, index, part, (nearer < z) & (z < LINE - 1), (nearer > z) & (z > 0)
            )
            near_act(order[index - 1], part)

    next_act(1)
    for k in range(1, LINE):
        pump(1, k)
    pump_down(1)
    next_act(2)

    def hid_piece(place, source):
        return hidden.at[
            pl.ds(pl.multiple_of(place * rows, rows), rows),
            pl.ds(pl.multiple_of(source * units, units), units),
        ]

    def gated(index):
        place = order[index]
        for part in range(PARTS):
            arrived(act_piece(place, col_flips[1], part), act_spread_recv.at[place, 0, part])
            arrived(act_piece(place, col_flips[3], part), act_spread_recv.at[place, 2, part])
        here = pl.ds(pl.multiple_of(place * rows, rows), rows)
        both = jnp.dot(act[here, :], gate_up[...], preferred_element_type=jnp.float32)
        gate = both[:, :units]
        hidden[here, pl.ds(pl.multiple_of(z * units, units), units)] = (
            gate / (1.0 + jnp.exp(-gate)) * both[:, units:]
        ).astype(jnp.bfloat16)

    def leave(index):
        place = order[index]
        piece = hid_piece(place, z)
        up_line(piece, piece, hid_send.at[index, 0], hid_recv.at[place, z], z < LINE - 1)
        down_line(piece, piece, hid_send.at[index, 1], hid_recv.at[place, z], z > 0)

    def pass_hidden(index, distance):
        for side, source, when in (
            (0, z - distance, (z - distance >= 0) & (z < LINE - 1)),
            (1, z + distance, (z + distance < LINE) & (z > 0)),
        ):
            source = (source + LINE) % LINE
            place = arrival(source)[index]
            piece = hid_piece(place, source)
            copy = remote(
                piece, piece, hid_pass_send.at[index, distance - 1, side],
                hid_recv.at[place, source],
                sp=((rank + PAIR) if side == 0 else (rank + ranks - PAIR)) % ranks,
            )

            @pl.when(when)
            def _():
                arrived(piece, hid_recv.at[place, source])
                copy.start()

            pending.append((copy, when))

    upper = z // (LINE // 2)

    def row_place(index):
        return index * upper + (LINE - 1 - index) * (1 - upper)

    def hidden_all(index):
        place = row_place(index)
        for distance in range(1, LINE):
            for source, when in (
                (LINE - 1 - distance, z == LINE - 1),
                (distance, z == 0),
            ):

                @pl.when(when)
                def _():
                    arrived(hid_piece(place, source), hid_recv.at[place, source])

    def row_sems(index):
        return (
            core_rows_send.at[index], core_rows_recv.at[index], near_rows_send.at[index],
            near_rows_recv.at[index],
        )

    def start_rows(index):
        place = row_place(index)
        hidden_all(index)
        here = pl.ds(pl.multiple_of(place * rows, rows), rows)
        project(hidden[here, :], down, partial_rows.at[index])
        fold(
            partial_rows.at[index], core_rows.at[index], near_rows_out.at[index],
            near_rows_in.at[index], row_sems(index),
        )

    def end_rows(index):
        place = row_place(index)

        def keep(at, values):
            rows_out[index, :, at] = values.astype(jnp.bfloat16)

        folded(
            partial_rows.at[index], core_rows.at[index], near_rows_in.at[index], row_sems(index),
            keep,
        )
        send(
            remote(
                rows_out.at[index], rows_in.at[z], rows_send.at[index], rows_recv.at[z],
                sp=place * PAIR + x,
            ),
            z != place,
        )

        @pl.when(z == place)
        def _():
            rows_in[z] = rows_out[index]


    def weights_ready():
        for copy in own_copies:
            copy.wait()
        paired(0)
        paired(1)

    outer = (z == 0) | (z == LINE - 1)

    def early(first):
        weights_ready()
        for index in range(2):
            gated(index)
            place = order[index]
            piece = hid_piece(place, z)
            recv = hid_recv.at[place, z]
            up = remote(
                piece, piece, hid_send.at[index, 0], recv, sp=(rank + PAIR) % ranks
            )
            lower = remote(
                piece, piece, hid_send.at[index, 1], recv, sp=(rank + ranks - PAIR) % ranks
            )
            if first:
                pl.when(z == 0)(up.start)
                pl.when(z > 0)(lower.start)
            else:
                up.start()
                lower.start()

    pl.when(outer)(functools.partial(early, True))
    next_act(3)
    pl.when(inner > 0)(functools.partial(early, False))
    for index in range(2):
        piece = hid_piece(order[index], z)
        for side, when in ((0, z < LINE - 1), (1, z > 0)):
            pending.append(
                (remote(piece, piece, hid_send.at[index, side], hid_send.at[index, side],
                        sp=mate), when)
            )
    gated(2)
    leave(2)
    for part in range(PARTS):
        near_act(order[LINE - 1], part)
    gated(3)
    leave(3)
    pass_hidden(0, 1)
    pass_hidden(1, 1)
    pass_hidden(0, 2)
    pass_hidden(2, 1)
    pass_hidden(1, 2)
    pass_hidden(3, 1)
    pass_hidden(2, 2)
    pass_hidden(3, 2)
    for half in range(2):
        arrived(down.at[down_part(half), down_mate], down_recv.at[half])
    start_rows(0)
    start_rows(1)
    end_rows(0)
    start_rows(2)
    end_rows(1)
    start_rows(3)
    end_rows(2)
    end_rows(3)
    for source in range(LINE):

        @pl.when(z != source)
        def _():
            arrived(rows_in.at[source], rows_recv.at[source])

    part = rows_in.shape[2]
    for source in range(LINE):
        at = slice(source * part, (source + 1) * part)
        result_ref[:, at] = (
            middle[:, at].astype(jnp.float32) + rows_in[source].astype(jnp.float32)
        ).astype(jnp.bfloat16)

    for copy, when in pending:
        if when is None:
            copy.wait_send()
        else:
            pl.when(when)(copy.wait_send)

    def drain(source, carry):
        piece = lat_piece(source, col)
        for slot in range(COLUMNS - 1):
            remote(
                piece, piece, lat_spread_send.at[source, slot], lat_spread_send.at[source, slot],
                tp=col_flips[1],
            ).wait_send()
        return carry

    lax.fori_loop(0, rank + 1, drain, 0)

    def drain_onward(place, carry):
        lat_onward(place).wait_send()
        return carry

    lax.fori_loop(0, z, drain_onward, 0)


def fused_body(
    resid,
    queries,
    latent,
    rope_key,
    lat_gain,
    kv_weight,
    out_gain,
    out_weight,
    ffn_gain,
    gate_weight,
    up_weight,
    down_weight,
):
    ranks, columns = lax.axis_size("sp"), lax.axis_size("tp")
    rows, width = resid.shape
    share = rows // columns
    heads = queries.shape[1] // (NOPE + ROPE)
    units = gate_weight.shape[1] // LINE
    block = gate_weight.shape[0]
    depth = latent.shape[1]
    half = ROPE // 2
    inverse = THETA ** (-jnp.arange(half, dtype=jnp.float32) / half)
    inverse = jnp.concatenate([inverse, inverse]).reshape(1, ROPE)
    bf, f32 = jnp.bfloat16, jnp.float32
    dma = pltpu.SemaphoreType.DMA
    vmem = pl.BlockSpec(memory_space=pltpu.VMEM)
    anywhere = pl.BlockSpec(memory_space=pl.ANY)
    part = width // LINE
    others = columns - 1
    return pl.pallas_call(
        whole_step,
        out_shape=jax.ShapeDtypeStruct((share, width), bf),
        in_specs=[vmem] * 6 + [anywhere] * 7,
        out_specs=vmem,
        scratch_shapes=[
            pltpu.VMEM((share, depth + LANES), bf),
            pltpu.VMEM((share, ROPE), bf),
            pltpu.VMEM((ranks, rows, depth + LANES), bf),
            pltpu.VMEM((heads, rows, 2 * LANES), bf),
            pltpu.VMEM((share, width), bf),
            pltpu.VMEM(kv_weight.shape, bf),
            pltpu.VMEM(out_weight.shape, bf),
            pltpu.VMEM((ranks * block, 2 * units), bf),
            pltpu.VMEM((LINE * units, PAIR * down_weight.shape[1]), bf),
            pltpu.VMEM((LINE * rows, width), bf),
            pltpu.VMEM((LINE * rows, LINE * units), bf),
            pltpu.VMEM((heads, rows, LANES), f32),
            pltpu.VMEM((heads, rows, LANES), f32),
            pltpu.VMEM((rows, heads * VDIM), f32),
            pltpu.VMEM((rows, LANES), f32),
            pltpu.VMEM((others, share, LANES), f32),
            pltpu.VMEM((rows, width), bf),
            pltpu.VMEM((2, share, width), bf),
            pltpu.VMEM((share, width), bf),
            pltpu.VMEM((share, width), bf),
            pltpu.VMEM((LINE, rows, part), bf),
            pltpu.VMEM((LINE, 2, share, part), bf),
            pltpu.VMEM((LINE, share, part), bf),
            pltpu.VMEM((LINE, share, part), bf),
            pltpu.VMEM((LINE, share, part), bf),
            pltpu.VMEM((LINE, share, part), bf),
            pltpu.VMEM((share, width), bf),
            pltpu.VMEM((share, width), f32),
            dma((9,)),
            dma((LINE,)),
            dma((ranks,)),
            dma((LINE,)),
            dma((ranks, others)),
            dma((ranks, others)),
            dma((2, LINE)),
            dma((2, LINE)),
            dma((2, LINE)),
            dma((2, LINE)),
            dma((2,)),
            dma((2,)),
            dma((2 * LINE, PARTS)),
            dma((LINE, PARTS)),
            dma((LINE, others, PARTS)),
            dma((LINE, others, PARTS)),
            dma((others,)),
            dma((others,)),
            dma((2,)),
            dma((2,)),
            dma((1,)),
            dma((1,)),
            dma((LINE, 2)),
            dma((LINE, 2, 2)),
            dma((LINE, LINE)),
            dma((LINE, 2)),
            dma((LINE, 2)),
            dma((LINE,)),
            dma((LINE,)),
            dma((LINE,)),
            dma((LINE,)),
        ],
        compiler_params=pltpu.CompilerParams(
            collective_id=0, has_side_effects=True, vmem_limit_bytes=66 * 1024 * 1000
        ),
    )(
        queries,
        latent,
        inverse,
        lat_gain.reshape(1, -1),
        out_gain.reshape(1, -1),
        ffn_gain.reshape(1, -1),
        rope_key,
        resid,
        kv_weight,
        out_weight,
        gate_weight,
        up_weight,
        down_weight,
    )


def solution(mesh):
    placed = (
        P("sp", None),
        P("sp", "tp"),
        P("sp", None),
        P("sp", None),
        P(),
        P(None, "tp"),
        P("tp"),
        P("tp", None),
        P(),
        P("sp", "tp"),
        P("sp", "tp"),
        P("tp", "sp"),
    )

    def mapped(function):
        return jax.shard_map(
            function, mesh=mesh, in_specs=placed, out_specs=P(("sp", "tp"), None), check_vma=False
        )

    if mesh.shape["sp"] == PAIR * LINE and mesh.shape["tp"] == COLUMNS:
        return mapped(fused_body)
    return mapped(plain_body)
```

```python
import functools
import math

import jax
import jax.numpy as jnp
import numpy as np
from jax import lax
from jax.experimental import pallas as pl
from jax.experimental.pallas import tpu as pltpu
from jax.sharding import PartitionSpec as P


HEADS = 16
NOPE = 128
ROPE = 64
VDIM = 128


EPSILON = 1e-06
THETA = 10000.0
LOWEST = -1e30
GROUP = 4


def rotate(values, places):
    half = values.shape[-1] // 2
    inverse = THETA ** (-jnp.arange(half, dtype=jnp.float32) / half)
    angle = places[..., None] * inverse
    cosine = jnp.cos(angle)
    sine = jnp.sin(angle)
    first = values[..., :half]
    second = values[..., half:]
    return jnp.concatenate(
        [first * cosine - second * sine, first * sine + second * cosine], axis=-1
    )


def norm_rows(values, gain):
    wide = values.astype(jnp.float32)
    return wide * lax.rsqrt(jnp.mean(wide * wide, axis=-1, keepdims=True) + EPSILON) * gain


def make_keys(latent_piece, rotary_piece, lat_gain, kv_weight, key_index):
    normed = norm_rows(latent_piece, lat_gain).astype(jnp.bfloat16)
    key_value = jnp.dot(normed, kv_weight, preferred_element_type=jnp.float32)
    key_value = key_value.astype(jnp.bfloat16)
    key_rope = rotate(rotary_piece.astype(jnp.float32), key_index.astype(jnp.float32)).astype(
        jnp.bfloat16
    )
    return (key_value, key_rope)


def to_near(values, flip):
    ranks = lax.axis_size("sp")
    return lax.ppermute(values, "sp", [(rank, rank ^ flip) for rank in range(ranks)])


def to_high(values, step, ranks):
    if step % (ranks // GROUP) == 0:
        return values
    return lax.ppermute(
        values, "sp", [(rank, (rank + step * GROUP) % ranks) for rank in range(ranks)]
    )


def reorder(blocks, place):
    bit = 1
    while bit < len(blocks):
        swap = place // bit % 2 == 1
        blocks = [jnp.where(swap, blocks[j ^ bit], blocks[j]) for j in range(len(blocks))]
        bit *= 2
    return blocks


def by_distance(values, place):
    return jnp.concatenate(reorder(jnp.split(values, GROUP, axis=1), place), axis=1)


def to_column(values, bit):
    columns = lax.axis_size("tp")
    return lax.ppermute(values, "tp", [(column, column ^ bit) for column in range(columns)])


def gather_columns(values):
    rows = values.shape[0]
    held = {0: values}
    bit = lax.axis_size("tp") // 2
    while bit:
        keys = sorted(held)
        theirs = to_column(jnp.concatenate([held[key] for key in keys], axis=0), bit)
        for at, key in enumerate(keys):
            held[key + bit] = theirs[at * rows : (at + 1) * rows]
        bit //= 2
    return jnp.concatenate([held[key] for key in sorted(held)], axis=0)


def scatter_columns(values):
    columns = lax.axis_size("tp")
    blocks = dict(enumerate(jnp.split(values, columns, axis=0)))
    bit = 1
    while bit < columns:
        mine = [key for key in sorted(blocks) if not key & bit]
        theirs = to_column(jnp.concatenate([blocks[key + bit] for key in mine], axis=0), bit)
        theirs = jnp.split(theirs, len(mine), axis=0)
        blocks = {
            key: (blocks[key].astype(jnp.float32) + piece.astype(jnp.float32)).astype(jnp.bfloat16)
            for key, piece in zip(mine, theirs)
        }
        bit *= 2
    return blocks[0]


def near_weights(gate, up, down):
    gate_one = to_near(gate, 1)
    up_two = to_near(up, 2)
    up_one = to_near(up, 1)
    gate_two = to_near(gate, 2)
    gate_both = to_near(gate_one, 2)
    up_both = to_near(up_two, 1)
    down, gate_both, up_both = lax.optimization_barrier((down, gate_both, up_both))
    half = down.shape[0] // 2
    down_one = to_near(down, 1)
    down_two = to_near(down, 2)
    far = [to_near(down_one[:half], 2), to_near(down_two[half:], 1)]
    down_both = jnp.concatenate(far, axis=0)
    return (
        (gate, gate_one, gate_two, gate_both),
        (up, up_one, up_two, up_both),
        (down, down_one, down_two, down_both),
    )


def blocks_dot(rows, weights, block):
    return sum(
        jnp.dot(
            rows[:, place * block : (place + 1) * block], weight, preferred_element_type=jnp.float32
        )
        for place, weight in enumerate(weights)
    )


def plain_body(
    resid,
    queries,
    latent,
    rope_key,
    lat_gain,
    kv_weight,
    out_gain,
    out_weight,
    ffn_gain,
    gate_weight,
    up_weight,
    down_weight,
):
    gate_blocks, up_blocks, down_blocks = near_weights(gate_weight, up_weight, down_weight)
    rows_here = resid.shape[0]
    first_row = lax.axis_index("sp") * rows_here
    heads_here = queries.shape[1] // (NOPE + ROPE)
    columns = lax.axis_size("tp")
    column = lax.axis_index("tp")
    share = rows_here // columns
    query = jnp.concatenate(reorder(jnp.split(queries, columns, axis=0), column), axis=0)
    query = query.reshape(rows_here, heads_here, NOPE + ROPE)
    within = jnp.arange(rows_here, dtype=jnp.int32)
    own_columns = (within // share) ^ column
    query_index = first_row + own_columns * share + within % share
    query_nope = query[:, :, :NOPE]
    query_rope = rotate(
        query[:, :, NOPE:].astype(jnp.float32), query_index.astype(jnp.float32)[:, None]
    ).astype(jnp.bfloat16)
    scale = 1.0 / math.sqrt(NOPE + ROPE)

    def accumulate(state, key_value, key_rope):
        running_max, running_sum, weighted = state
        length = key_value.shape[0]
        key_value = key_value.reshape(length, heads_here, NOPE + VDIM)
        scores = jnp.einsum(
            "qhd,khd->hqk", query_nope, key_value[:, :, :NOPE], preferred_element_type=jnp.float32
        )
        scores = (
            scores
            + jnp.einsum("qhr,kr->hqk", query_rope, key_rope, preferred_element_type=jnp.float32)
        ) * scale
        allowed = (key_index[None, :] <= query_index[:, None])[None]
        scores = jnp.where(allowed, scores, LOWEST)
        new_max = jnp.maximum(running_max, jnp.max(scores, axis=-1))
        weights = jnp.where(allowed, jnp.exp(scores - new_max[:, :, None]), 0.0)
        running_sum = jnp.sum(weights, axis=-1)
        added = jnp.einsum(
            "hqk,khd->qhd",
            weights.astype(jnp.bfloat16),
            key_value[:, :, NOPE:],
            preferred_element_type=jnp.float32,
        )
        weighted = added
        return (new_max, running_sum, weighted)

    initial = (
        jnp.full((heads_here, rows_here), LOWEST, jnp.float32),
        jnp.zeros((heads_here, rows_here), jnp.float32),
        jnp.zeros((rows_here, heads_here, VDIM), jnp.float32),
    )
    ranks = lax.axis_size("sp")
    rank = lax.axis_index("sp")
    both = jnp.concatenate([latent, rope_key], axis=1)
    both = lax.dynamic_slice_in_dim(both, column * share, share, 0)
    pieces = [both]
    for step in range(1, ranks):
        onward = [(source, source + step) for source in range(ranks - step)]
        pieces.append(lax.ppermute(both, "sp", onward))
    both = gather_columns(jnp.concatenate(pieces, axis=0))
    within = jnp.arange(both.shape[0], dtype=jnp.int32)
    source = (rank - within // share % ranks + ranks) % ranks
    key_index = source * rows_here + ((within // (share * ranks)) ^ column) * share + within % share
    pieces = (both[:, : latent.shape[1]], both[:, latent.shape[1] :])

    def update(state):
        key_value, key_rope = make_keys(pieces[0], pieces[1], lat_gain, kv_weight, key_index)
        return accumulate(state, key_value, key_rope)

    _, running_sum, weighted = update(initial)
    attended = (weighted / jnp.transpose(running_sum)[:, :, None]).astype(jnp.bfloat16)
    attended_float = attended.reshape(rows_here, heads_here * VDIM).astype(jnp.float32)
    squares = jnp.split(jnp.sum(attended_float * attended_float, axis=1), columns)
    squares = lax.psum(jnp.concatenate(reorder(squares, column)), "tp")
    squares = jnp.concatenate(reorder(jnp.split(squares, columns), column))
    normed_out = attended_float * lax.rsqrt(squares / (HEADS * VDIM) + EPSILON)[:, None] * out_gain
    normed_out = normed_out.astype(jnp.bfloat16)
    own_first = lax.axis_index("tp") * share
    projected = jnp.dot(normed_out, out_weight, preferred_element_type=jnp.float32)
    projected = projected.astype(jnp.bfloat16)
    attn_sum = scatter_columns(projected).astype(jnp.float32)
    own_resid = lax.dynamic_slice_in_dim(resid, own_first, share, 0)
    middle = (own_resid.astype(jnp.float32) + attn_sum).astype(jnp.bfloat16)
    highs = ranks // GROUP
    high = rank // GROUP
    place = rank % GROUP
    width = resid.shape[1]
    block = width // ranks
    wide = GROUP * block
    mids = norm_rows(middle, ffn_gain).astype(jnp.bfloat16)
    mids = [
        to_high(
            by_distance(
                lax.dynamic_slice_in_dim(mids, (high + step) % highs * wide, wide, 1), place
            ),
            step,
            ranks,
        )
        for step in range(highs)
    ]
    mids = [gather_columns(piece) for piece in mids]
    gates, ups = None, None
    for step in list(range(1, highs)) + [0]:
        piece = mids[step]
        gate = blocks_dot(piece, gate_blocks, block)
        up = blocks_dot(piece, up_blocks, block)
        if step:
            gate = to_high(gate.astype(jnp.bfloat16), highs - step, ranks).astype(jnp.float32)
            up = to_high(up.astype(jnp.bfloat16), highs - step, ranks).astype(jnp.float32)
        gates = gate if gates is None else gates + gate
        ups = up if ups is None else ups + up
    hidden = (jax.nn.silu(gates) * ups).astype(jnp.bfloat16)
    received = [to_high(hidden, step, ranks) for step in range(highs)]
    terms = []
    for step in range(highs):
        partial = jnp.concatenate(
            [
                jnp.dot(received[step], weight, preferred_element_type=jnp.float32).astype(
                    jnp.bfloat16
                )
                for weight in down_blocks
            ],
            axis=1,
        )
        partial = to_high(scatter_columns(partial), highs - step, ranks)
        terms.append(by_distance(partial, place))
    terms = jnp.concatenate(terms, axis=1)
    ffn_sum = jnp.concatenate(
        [
            lax.dynamic_slice_in_dim(terms, (index - high + highs) % highs * wide, wide, 1)
            for index in range(highs)
        ],
        axis=1,
    ).astype(jnp.float32)
    return (middle.astype(jnp.float32) + ffn_sum).astype(jnp.bfloat16)


LANES = 128
PAIR = 2
LINE = 4
COLUMNS = 4
MESH = pl.DeviceIdType.MESH


PARTS = 4


def whole_step(
    inverse_ref,
    lat_gain_ref,
    out_gain_ref,
    ffn_gain_ref,
    query_hbm,
    latent_hbm,
    rope_hbm,
    resid_hbm,
    kv_hbm,
    out_hbm,
    gate_hbm,
    up_hbm,
    down_hbm,
    result_ref,
    lat_mine,
    rope_mine,
    rope_wide,
    wide_mine,
    query_ref,
    lat_buf,
    query,
    resid,
    kv_w,
    out_w,
    gate_up,
    down,
    act,
    hidden,
    top,
    norm,
    acc,
    stats_mine,
    stats_in,
    partial,
    core_in,
    near_out,
    near_in,
    partial_rows,
    core_rows,
    near_rows_out,
    near_rows_in,
    rows_out,
    rows_in,
    middle,
    total,
    local_sem,
    lat_send,
    lat_recv,
    lat_pass_send,
    lat_spread_send,
    lat_spread_recv,
    turn_send,
    turn_recv,
    pair_send,
    pair_recv,
    down_send,
    down_recv,
    act_line_send,
    act_line_recv,
    act_spread_send,
    act_spread_recv,
    stat_send,
    stat_recv,
    core_send,
    core_recv,
    near_send,
    near_recv,
    hid_send,
    hid_pass_send,
    hid_recv,
    core_rows_send,
    core_rows_recv,
    near_rows_send,
    near_rows_recv,
    rows_send,
    rows_recv,
):
    rank = lax.axis_index("sp")
    col = lax.axis_index("tp")
    ranks = lat_buf.shape[0]
    rows = lat_buf.shape[1]
    share = lat_mine.shape[0]
    width = resid.shape[1]
    units = hidden.shape[1] // LINE
    block = gate_hbm.shape[0]
    latent = kv_w.shape[0]
    heads = query.shape[0]
    z = rank // PAIR
    x = rank % PAIR
    mate = z * PAIR + (PAIR - 1 - x)
    inner = ((z + 1) // 2) % 2
    z_flips = [z, z + 1 - 2 * (z % 2), (z + 2) % LINE, LINE - 1 - z]
    col_flips = [col, col + 1 - 2 * (col % 2), (col + 2) % COLUMNS, COLUMNS - 1 - col]
    pending = []

    def remote(src, dst, send, recv, sp=None, tp=None):
        target = (rank if sp is None else sp, col if tp is None else tp)
        return pltpu.make_async_remote_copy(
            src_ref=src, dst_ref=dst, send_sem=send, recv_sem=recv, device_id=target,
            device_id_type=MESH,
        )

    def arrived(dst, recv):
        remote(dst, dst, recv, recv, tp=col_flips[1]).wait_recv()

    def send(copy, when=None):
        if when is None:
            copy.start()
        else:
            pl.when(when)(copy.start)
        pending.append((copy, when))

    def local(src, dst, slot):
        copy = pltpu.make_async_copy(src, dst, local_sem.at[slot])
        copy.start()
        return copy

    own_rows = pl.ds(pl.multiple_of(col * share, share), share)
    wide_copy = local(latent_hbm.at[own_rows, :], wide_mine, 9)
    rope_copy = local(rope_hbm, rope_mine, 8)
    barrier = pltpu.get_barrier_semaphore()
    for step in range(1, ranks):
        pl.semaphore_signal(
            barrier, inc=1, device_id=((rank + step) % ranks, col), device_id_type=MESH
        )
    for flip in col_flips[1:]:
        pl.semaphore_signal(barrier, inc=1, device_id=(rank, flip), device_id_type=MESH)
    query_copy = local(query_hbm, query_ref, 10)
    kv_copy = local(kv_hbm, kv_w, 0)
    out_copy = local(out_hbm, out_w, 1)
    resid_copy = local(resid_hbm.at[own_rows, :], resid, 2)

    def turned(values, cosine, sine):
        half = values.shape[1] // 2
        swapped = jnp.concatenate([values[:, half:], values[:, :half]], axis=1)
        return values * cosine + swapped * sine

    def table(start, count):
        shape = (count, ROPE)
        place = (start + lax.broadcasted_iota(jnp.int32, shape, 0)).astype(jnp.float32)
        angle = place * inverse_ref[...]
        sine = jnp.sin(angle)
        low = lax.broadcasted_iota(jnp.int32, shape, 1) < ROPE // 2
        return jnp.cos(angle), jnp.where(low, -sine, sine)

    cosine, sine = table(rank * rows + col * share, share)
    wide_copy.wait()
    wide = wide_mine[...].astype(jnp.float32)
    wide = wide * lax.rsqrt(jnp.mean(wide * wide, axis=1, keepdims=True) + EPSILON)
    lat_mine[:, :latent] = (wide * lat_gain_ref[...]).astype(jnp.bfloat16)
    rope_copy.wait()
    rope_wide[...] = jnp.transpose(rope_mine[...].astype(jnp.float32))
    key_rope = turned(rope_wide[own_rows, :], cosine, sine).astype(jnp.bfloat16)
    lat_mine[:, latent:] = jnp.concatenate([key_rope, jnp.zeros_like(key_rope)], axis=1)

    pl.semaphore_wait(barrier, ranks - 1 + COLUMNS - 1)

    def lat_piece(source, column):
        return lat_buf.at[source, pl.ds(pl.multiple_of(column * share, share), share), :]

    def lat_spread(source, piece, flip, slot):
        return remote(
            piece, lat_piece(source, col_flips[slot - flip]),
            lat_spread_send.at[source, slot - 1], lat_spread_recv.at[source, slot - 1],
            tp=col_flips[flip],
        )

    for step in range(1, LINE):
        send(
            remote(
                lat_mine, lat_piece(rank, col), lat_send.at[step - 1], lat_recv.at[rank],
                sp=(rank + PAIR * step) % ranks,
            ),
            z + step < LINE,
        )
    send(
        remote(
            lat_mine, lat_piece(rank, col), lat_send.at[LINE - 1], lat_recv.at[rank], sp=mate
        ),
        x == 0,
    )
    lat_spread(rank, lat_mine, 2, 2).start()
    lat_spread(rank, lat_mine, 1, 1).start()
    lat_buf[rank, own_rows, :] = lat_mine[...]

    def region(kind, source):
        at = pl.multiple_of(source * block, block)
        return gate_up.at[pl.ds(at, block), pl.ds(kind * units, units)]

    def own_part(kind, place):
        at = pl.multiple_of(place * units, units)
        return (gate_hbm, up_hbm)[kind].at[:, pl.ds(at, units)]

    def down_part(half):
        middle_row = down_hbm.shape[0] // 2
        return pl.ds(half * middle_row, middle_row)

    def turn(kind):
        for k in range(1, LINE):
            send(
                remote(
                    own_part(kind, z_flips[k]), region(kind, rank), turn_send.at[kind, k],
                    turn_recv.at[kind, k], sp=z_flips[k] * PAIR + x,
                )
            )

    def pump(kind, k):
        here = region(kind, z_flips[k] * PAIR + x)
        if k:
            arrived(here, turn_recv.at[kind, k])
        send(
            remote(
                here if k else own_part(kind, z), here, pair_send.at[kind, k],
                pair_recv.at[kind, k], sp=mate,
            )
        )

    def paired(kind):
        for k in range(LINE):
            arrived(region(kind, z_flips[k] * PAIR + (PAIR - 1 - x)), pair_recv.at[kind, k])

    down_own = pl.ds(pl.multiple_of(x * down_hbm.shape[1], LANES), down_hbm.shape[1])
    down_mate = pl.ds(
        pl.multiple_of((PAIR - 1 - x) * down_hbm.shape[1], LANES), down_hbm.shape[1]
    )

    def pump_down(half):
        send(
            remote(
                down_hbm.at[down_part(half), :], down.at[down_part(half), down_own],
                down_send.at[half], down_recv.at[half], sp=mate,
            )
        )

    turn(0)
    turn(1)
    own_pumps = []
    own_copies = [local(own_part(kind, z), region(kind, rank), 3 + kind) for kind in range(2)]
    own_copies.append(local(down_hbm, down.at[:, down_own], 5))

    cosine, sine = table(rank * rows, rows)
    query_copy.wait()
    for head in range(heads):
        at = head * (NOPE + ROPE)
        rotary = turned(
            query_ref[:, at + NOPE : at + NOPE + ROPE].astype(jnp.float32), cosine, sine
        ).astype(jnp.bfloat16)
        query[head, :, :NOPE] = query_ref[:, at : at + NOPE]
        query[head, :, NOPE:] = jnp.concatenate([rotary, jnp.zeros_like(rotary)], axis=1)
    top[...] = jnp.full(top.shape, LOWEST, jnp.float32)
    norm[...] = jnp.zeros(norm.shape, jnp.float32)
    acc[...] = jnp.zeros(acc.shape, jnp.float32)
    scale = math.log2(math.e) / math.sqrt(NOPE + ROPE)
    kv_copy.wait()

    def lat_taken(source):
        piece = lat_piece(source, col)
        arrived(piece, lat_recv.at[source])
        lat_spread(source, piece, 2, 2).start()
        lat_spread(source, piece, 1, 1).start()

    def lat_onward(place):
        piece = lat_piece(place * PAIR + x, col)
        return remote(
            piece, piece, lat_pass_send.at[place], lat_recv.at[place * PAIR + x], sp=mate
        )

    for kind in range(2):
        here = region(kind, rank)
        own_pumps.append(
            remote(
                own_part(kind, z), here, pair_send.at[kind, 0], pair_recv.at[kind, 0], sp=mate
            )
        )
    own_pumps.append(
        remote(
            down_hbm.at[down_part(0), :], down.at[down_part(0), down_own], down_send.at[0],
            down_recv.at[0], sp=mate,
        )
    )
    pending += [(copy, None) for copy in own_pumps]

    def attend(index, carry):
        source = rank - index

        @pl.when((index < rank) & ((source - 1) % PAIR != x) & (index + x > 0))
        def _():
            lat_taken(source - 1)

        arrived(lat_piece(source, col_flips[2]), lat_spread_recv.at[source, 1])
        lat_spread(source, lat_piece(source, col_flips[2]), 1, 3).start()
        arrived(lat_piece(source, col_flips[1]), lat_spread_recv.at[source, 0])
        arrived(lat_piece(source, col_flips[3]), lat_spread_recv.at[source, 2])
        key_value = jnp.dot(
            lat_buf[source, :, :latent], kv_w[...], preferred_element_type=jnp.float32
        ).astype(jnp.bfloat16)
        key_rope = lat_buf[source, :, latent:]
        row_of = lax.broadcasted_iota(jnp.int32, (rows, rows), 0) + index * rows
        allowed = lax.broadcasted_iota(jnp.int32, (rows, rows), 1) <= row_of
        for head in range(heads):
            at = head * (NOPE + VDIM)
            keys = jnp.concatenate([key_value[:, at : at + NOPE], key_rope], axis=1)
            scores = lax.dot_general(
                query[head], keys, (((1,), (1,)), ((), ())), preferred_element_type=jnp.float32
            )
            scores = jnp.where(allowed, scores * scale, LOWEST)
            old = top[head]
            new = jnp.maximum(old, jnp.max(scores, axis=1, keepdims=True))
            weights = jnp.exp2(scores - new[:, :1])
            fade = jnp.exp2(old - new)
            top[head] = new
            norm[head] = norm[head] * fade + jnp.sum(weights, axis=1, keepdims=True)
            across = slice(head * VDIM, (head + 1) * VDIM)
            acc[:, across] = acc[:, across] * fade + jnp.dot(
                weights.astype(jnp.bfloat16), key_value[:, at + NOPE : at + NOPE + VDIM],
                preferred_element_type=jnp.float32,
            )

        @pl.when(index == 0)
        def _():
            def onward(step, carry):
                lat_taken((z - 1 - step) * PAIR + x)
                lat_onward(z - 1 - step).start()
                return carry

            lax.fori_loop(0, z, onward, 0)

            @pl.when((x == 0) & (rank > 0))
            def _():
                lat_taken(rank - 1)

            for copy in own_pumps:
                copy.start()

        return carry

    lax.fori_loop(0, rank + 1, attend, 0)

    squares = jnp.zeros((rows, 1), jnp.float32)
    attended = []
    for head in range(heads):
        across = slice(head * VDIM, (head + 1) * VDIM)
        part = (acc[:, across] / norm[head]).astype(jnp.bfloat16).astype(jnp.float32)
        squares = squares + jnp.sum(part * part, axis=1, keepdims=True)
        attended.append((part * out_gain_ref[:, across]).astype(jnp.bfloat16))
    attended = jnp.concatenate(attended, axis=1)
    stats_mine[...] = jnp.broadcast_to(squares, stats_mine.shape)

    chunk = 4 * LANES

    def piece_of(ref, column):
        return ref.at[pl.ds(pl.multiple_of(column * share, share), share), :]

    def project(left, right, target):
        def one(index, carry):
            at = pl.ds(pl.multiple_of(index * chunk, chunk), chunk)
            target[:, at] = jnp.dot(
                left, right[:, at], preferred_element_type=jnp.float32
            ).astype(jnp.bfloat16)
            return carry

        lax.fori_loop(0, right.shape[1] // chunk, one, 0)

    def each_chunk(across, work):
        def one(index, carry):
            work(pl.ds(pl.multiple_of(index * chunk, chunk), chunk))
            return carry

        lax.fori_loop(0, across // chunk, one, 0)

    def fold(part, core, out, near, sems):
        core_s, core_r, near_s, near_r = sems
        for slot, column in ((1, 3), (0, 1)):
            send(
                remote(
                    piece_of(part, col_flips[column]), core.at[slot], core_s.at[slot],
                    core_r.at[slot], tp=col_flips[1],
                )
            )
        arrived(core.at[1], core_r.at[1])
        theirs = pl.ds(pl.multiple_of(col_flips[2] * share, share), share)

        def add(at):
            out[:, at] = (
                part[theirs, at].astype(jnp.float32) + core[1, :, at].astype(jnp.float32)
            ).astype(jnp.bfloat16)

        each_chunk(out.shape[1], add)
        send(remote(out, near, near_s, near_r, tp=col_flips[2]))
        arrived(core.at[0], core_r.at[0])

    def folded(part, core, near, sems, keep):
        arrived(near, sems[3])

        def add(at):
            keep(
                at,
                part[own_rows, at].astype(jnp.float32)
                + core[0, :, at].astype(jnp.float32)
                + near[:, at].astype(jnp.float32),
            )

        each_chunk(near.shape[1], add)

    out_copy.wait()
    for m in range(1, COLUMNS):
        send(
            remote(
                stats_mine.at[pl.ds(pl.multiple_of(col_flips[m] * share, share), share), :],
                stats_in.at[m - 1], stat_send.at[m - 1], stat_recv.at[m - 1], tp=col_flips[m],
            )
        )
    project(attended, out_w, partial)
    first = (core_send, core_recv, near_send.at[0], near_recv.at[0])
    fold(partial, core_in, near_out, near_in, first)
    pump(0, 1)
    squares = stats_mine[own_rows, :]
    for m in range(1, COLUMNS):
        arrived(stats_in.at[m - 1], stat_recv.at[m - 1])
        squares = squares + stats_in[m - 1]
    factor = lax.rsqrt(squares / (HEADS * VDIM) + EPSILON)[:, :1]

    def keep_total(at, values):
        total[:, at] = values

    folded(partial, core_in, near_in, first, keep_total)
    resid_copy.wait()
    squares = jnp.zeros((share, 1), jnp.float32)
    for index in range(width // chunk):
        at = slice(index * chunk, (index + 1) * chunk)
        mid = (resid[:, at].astype(jnp.float32) + total[:, at] * factor).astype(jnp.bfloat16)
        middle[:, at] = mid
        mid = mid.astype(jnp.float32)
        squares = squares + jnp.sum(mid * mid, axis=1, keepdims=True)
    factor = lax.rsqrt(squares / width + EPSILON)

    slab = width // PARTS

    def act_piece(place, column, part):
        at = pl.multiple_of(place * rows + column * share, share)
        return act.at[pl.ds(at, share), pl.ds(part * slab, slab)]

    at_own = pl.ds(pl.multiple_of(z * rows + col * share, share), share)
    for index in range(width // chunk):
        at = slice(index * chunk, (index + 1) * chunk)
        act[at_own, at] = (
            middle[:, at].astype(jnp.float32) * factor * ffn_gain_ref[:, at]
        ).astype(jnp.bfloat16)

    def up_line(src, dst, send_sem, recv_sem, when):
        send(remote(src, dst, send_sem, recv_sem, sp=(rank + PAIR) % ranks), when)

    def down_line(src, dst, send_sem, recv_sem, when):
        send(remote(src, dst, send_sem, recv_sem, sp=(rank + ranks - PAIR) % ranks), when)

    def act_spread(place, flip, slot, part):
        piece = act_piece(place, col_flips[slot - flip], part)
        send(
            remote(
                piece, piece, act_spread_send.at[place, slot - 1, part],
                act_spread_recv.at[place, slot - 1, part], tp=col_flips[flip],
            )
        )

    def act_line(place, index, part, up, lower):
        piece = act_piece(place, col, part)
        recv = act_line_recv.at[place, part]
        up_line(piece, piece, act_line_send.at[2 * index, part], recv, up)
        down_line(piece, piece, act_line_send.at[2 * index + 1, part], recv, lower)
        act_spread(place, 2, 2, part)
        act_spread(place, 1, 1, part)

    for part in range(PARTS):
        act_line(z, 0, part, z < LINE - 1, z > 0)
    pump(0, 2)
    pump(0, 3)

    def arrival(at):
        inside = ((at + 1) // 2) % 2
        half, mirror = (at + 2) % LINE, LINE - 1 - at
        return [
            at,
            at + 1 - 2 * (at % 2),
            half * (1 - inside) + mirror * inside,
            mirror * (1 - inside) + half * inside,
        ]

    order = arrival(z)

    def near_act(place, part):
        arrived(act_piece(place, col_flips[2], part), act_spread_recv.at[place, 1, part])
        act_spread(place, 1, 3, part)

    def next_act(index):
        nearer = order[index]
        for part in range(PARTS):
            arrived(act_piece(nearer, col, part), act_line_recv.at[nearer, part])
            act_line(
                nearer, index, part, (nearer < z) & (z < LINE - 1), (nearer > z) & (z > 0)
            )
            near_act(order[index - 1], part)

    next_act(1)
    for k in range(1, LINE):
        pump(1, k)
    pump_down(1)
    next_act(2)

    def hid_piece(place, source):
        return hidden.at[
            pl.ds(pl.multiple_of(place * rows, rows), rows),
            pl.ds(pl.multiple_of(source * units, units), units),
        ]

    def gated(index):
        place = order[index]
        for part in range(PARTS):
            arrived(act_piece(place, col_flips[1], part), act_spread_recv.at[place, 0, part])
            arrived(act_piece(place, col_flips[3], part), act_spread_recv.at[place, 2, part])
        here = pl.ds(pl.multiple_of(place * rows, rows), rows)
        both = jnp.dot(act[here, :], gate_up[...], preferred_element_type=jnp.float32)
        gate = both[:, :units]
        hidden[here, pl.ds(pl.multiple_of(z * units, units), units)] = (
            gate / (1.0 + jnp.exp(-gate)) * both[:, units:]
        ).astype(jnp.bfloat16)

    def leave(index):
        place = order[index]
        piece = hid_piece(place, z)
        up_line(piece, piece, hid_send.at[index, 0], hid_recv.at[place, z], z < LINE - 1)
        down_line(piece, piece, hid_send.at[index, 1], hid_recv.at[place, z], z > 0)

    def pass_hidden(index, distance):
        for side, source, when in (
            (0, z - distance, (z - distance >= 0) & (z < LINE - 1)),
            (1, z + distance, (z + distance < LINE) & (z > 0)),
        ):
            source = (source + LINE) % LINE
            place = arrival(source)[index]
            piece = hid_piece(place, source)
            copy = remote(
                piece, piece, hid_pass_send.at[index, distance - 1, side],
                hid_recv.at[place, source],
                sp=((rank + PAIR) if side == 0 else (rank + ranks - PAIR)) % ranks,
            )

            @pl.when(when)
            def _():
                arrived(piece, hid_recv.at[place, source])
                copy.start()

            pending.append((copy, when))

    upper = z // (LINE // 2)

    def row_place(index):
        return index * upper + (LINE - 1 - index) * (1 - upper)

    def hidden_all(index):
        place = row_place(index)
        for distance in range(1, LINE):
            for source, when in (
                (LINE - 1 - distance, z == LINE - 1),
                (distance, z == 0),
            ):

                @pl.when(when)
                def _():
                    arrived(hid_piece(place, source), hid_recv.at[place, source])

    def row_sems(index):
        return (
            core_rows_send.at[index], core_rows_recv.at[index], near_rows_send.at[index],
            near_rows_recv.at[index],
        )

    def start_rows(index):
        place = row_place(index)
        hidden_all(index)
        here = pl.ds(pl.multiple_of(place * rows, rows), rows)
        project(hidden[here, :], down, partial_rows.at[index])
        fold(
            partial_rows.at[index], core_rows.at[index], near_rows_out.at[index],
            near_rows_in.at[index], row_sems(index),
        )

    def end_rows(index):
        place = row_place(index)

        def keep(at, values):
            rows_out[index, :, at] = values.astype(jnp.bfloat16)

        folded(
            partial_rows.at[index], core_rows.at[index], near_rows_in.at[index], row_sems(index),
            keep,
        )
        send(
            remote(
                rows_out.at[index], rows_in.at[z], rows_send.at[index], rows_recv.at[z],
                sp=place * PAIR + x,
            ),
            z != place,
        )

        @pl.when(z == place)
        def _():
            rows_in[z] = rows_out[index]


    def weights_ready():
        for copy in own_copies:
            copy.wait()
        paired(0)
        paired(1)

    outer = (z == 0) | (z == LINE - 1)

    def early(first):
        weights_ready()
        for index in range(2):
            gated(index)
            place = order[index]
            piece = hid_piece(place, z)
            recv = hid_recv.at[place, z]
            up = remote(
                piece, piece, hid_send.at[index, 0], recv, sp=(rank + PAIR) % ranks
            )
            lower = remote(
                piece, piece, hid_send.at[index, 1], recv, sp=(rank + ranks - PAIR) % ranks
            )
            if first:
                pl.when(z == 0)(up.start)
                pl.when(z > 0)(lower.start)
            else:
                up.start()
                lower.start()

    pl.when(outer)(functools.partial(early, True))
    next_act(3)
    pl.when(inner > 0)(functools.partial(early, False))
    for index in range(2):
        piece = hid_piece(order[index], z)
        for side, when in ((0, z < LINE - 1), (1, z > 0)):
            pending.append(
                (remote(piece, piece, hid_send.at[index, side], hid_send.at[index, side],
                        sp=mate), when)
            )
    gated(2)
    leave(2)
    for part in range(PARTS):
        near_act(order[LINE - 1], part)
    gated(3)
    leave(3)
    pass_hidden(0, 1)
    pass_hidden(1, 1)
    pass_hidden(0, 2)
    pass_hidden(2, 1)
    pass_hidden(1, 2)
    pass_hidden(3, 1)
    pass_hidden(2, 2)
    pass_hidden(3, 2)
    for half in range(2):
        arrived(down.at[down_part(half), down_mate], down_recv.at[half])
    start_rows(0)
    start_rows(1)
    end_rows(0)
    start_rows(2)
    end_rows(1)
    start_rows(3)
    end_rows(2)
    end_rows(3)
    for source in range(LINE):

        @pl.when(z != source)
        def _():
            arrived(rows_in.at[source], rows_recv.at[source])

    part = rows_in.shape[2]
    for source in range(LINE):
        at = slice(source * part, (source + 1) * part)
        result_ref[:, at] = (
            middle[:, at].astype(jnp.float32) + rows_in[source].astype(jnp.float32)
        ).astype(jnp.bfloat16)

    for copy, when in pending:
        if when is None:
            copy.wait_send()
        else:
            pl.when(when)(copy.wait_send)

    def drain(source, carry):
        piece = lat_piece(source, col)
        for slot in range(COLUMNS - 1):
            remote(
                piece, piece, lat_spread_send.at[source, slot], lat_spread_send.at[source, slot],
                tp=col_flips[1],
            ).wait_send()
        return carry

    lax.fori_loop(0, rank + 1, drain, 0)

    def drain_onward(place, carry):
        lat_onward(place).wait_send()
        return carry

    lax.fori_loop(0, z, drain_onward, 0)


def fused_body(
    resid,
    queries,
    latent,
    rope_key,
    lat_gain,
    kv_weight,
    out_gain,
    out_weight,
    ffn_gain,
    gate_weight,
    up_weight,
    down_weight,
):
    ranks, columns = lax.axis_size("sp"), lax.axis_size("tp")
    rows, width = resid.shape
    share = rows // columns
    heads = queries.shape[1] // (NOPE + ROPE)
    units = gate_weight.shape[1] // LINE
    block = gate_weight.shape[0]
    depth = latent.shape[1]
    half = ROPE // 2
    inverse = np.power(np.float32(THETA), -np.arange(half, dtype=np.float32) / np.float32(half))
    inverse = jnp.asarray(np.concatenate([inverse, inverse]).reshape(1, ROPE), jnp.float32)
    bf, f32 = jnp.bfloat16, jnp.float32
    dma = pltpu.SemaphoreType.DMA
    vmem = pl.BlockSpec(memory_space=pltpu.VMEM)
    anywhere = pl.BlockSpec(memory_space=pl.ANY)
    part = width // LINE
    others = columns - 1
    return pl.pallas_call(
        whole_step,
        out_shape=jax.ShapeDtypeStruct((share, width), bf),
        in_specs=[vmem] * 4 + [anywhere] * 9,
        out_specs=vmem,
        scratch_shapes=[
            pltpu.VMEM((share, depth + LANES), bf),
            pltpu.VMEM((ROPE, rows), bf),
            pltpu.VMEM((rows, ROPE), f32),
            pltpu.VMEM((share, depth), bf),
            pltpu.VMEM(queries.shape, bf),
            pltpu.VMEM((ranks, rows, depth + LANES), bf),
            pltpu.VMEM((heads, rows, 2 * LANES), bf),
            pltpu.VMEM((share, width), bf),
            pltpu.VMEM(kv_weight.shape, bf),
            pltpu.VMEM(out_weight.shape, bf),
            pltpu.VMEM((ranks * block, 2 * units), bf),
            pltpu.VMEM((LINE * units, PAIR * down_weight.shape[1]), bf),
            pltpu.VMEM((LINE * rows, width), bf),
            pltpu.VMEM((LINE * rows, LINE * units), bf),
            pltpu.VMEM((heads, rows, LANES), f32),
            pltpu.VMEM((heads, rows, LANES), f32),
            pltpu.VMEM((rows, heads * VDIM), f32),
            pltpu.VMEM((rows, LANES), f32),
            pltpu.VMEM((others, share, LANES), f32),
            pltpu.VMEM((rows, width), bf),
            pltpu.VMEM((2, share, width), bf),
            pltpu.VMEM((share, width), bf),
            pltpu.VMEM((share, width), bf),
            pltpu.VMEM((LINE, rows, part), bf),
            pltpu.VMEM((LINE, 2, share, part), bf),
            pltpu.VMEM((LINE, share, part), bf),
            pltpu.VMEM((LINE, share, part), bf),
            pltpu.VMEM((LINE, share, part), bf),
            pltpu.VMEM((LINE, share, part), bf),
            pltpu.VMEM((share, width), bf),
            pltpu.VMEM((share, width), f32),
            dma((11,)),
            dma((LINE,)),
            dma((ranks,)),
            dma((LINE,)),
            dma((ranks, others)),
            dma((ranks, others)),
            dma((2, LINE)),
            dma((2, LINE)),
            dma((2, LINE)),
            dma((2, LINE)),
            dma((2,)),
            dma((2,)),
            dma((2 * LINE, PARTS)),
            dma((LINE, PARTS)),
            dma((LINE, others, PARTS)),
            dma((LINE, others, PARTS)),
            dma((others,)),
            dma((others,)),
            dma((2,)),
            dma((2,)),
            dma((1,)),
            dma((1,)),
            dma((LINE, 2)),
            dma((LINE, 2, 2)),
            dma((LINE, LINE)),
            dma((LINE, 2)),
            dma((LINE, 2)),
            dma((LINE,)),
            dma((LINE,)),
            dma((LINE,)),
            dma((LINE,)),
        ],
        compiler_params=pltpu.CompilerParams(
            collective_id=0, has_side_effects=True, vmem_limit_bytes=66 * 1024 * 1000
        ),
    )(
        inverse,
        lat_gain.reshape(1, -1),
        out_gain.reshape(1, -1),
        ffn_gain.reshape(1, -1),
        queries,
        latent,
        rope_key.T,
        resid,
        kv_weight,
        out_weight,
        gate_weight,
        up_weight,
        down_weight,
    )


def solution(mesh):
    placed = (
        P("sp", None),
        P("sp", "tp"),
        P("sp", None),
        P("sp", None),
        P(),
        P(None, "tp"),
        P("tp"),
        P("tp", None),
        P(),
        P("sp", "tp"),
        P("sp", "tp"),
        P("tp", "sp"),
    )

    def mapped(function):
        return jax.shard_map(
            function, mesh=mesh, in_specs=placed, out_specs=P(("sp", "tp"), None), check_vma=False
        )

    if mesh.shape["sp"] == PAIR * LINE and mesh.shape["tp"] == COLUMNS:
        return mapped(fused_body)
    return mapped(plain_body)
```
